32 devices in a mesh: sp: 16 (over z, y, x), tp: 2 (over core).
Axes of the slice: x: 2, y: 2, z: 4, core: 2. Of those that a mesh axis runs over, the one named last changes fastest.
Arguments:
- queries: bfloat16 [4096, 1024], P('sp', 'tp'), may hold values from -6 to 6
- key_vectors: bfloat16 [4096, 1024], P('sp', 'tp'), may hold values from -6 to 6
- value_vectors: bfloat16 [4096, 1024], P('sp', 'tp'), may hold values from -6 to 6
- gate_inputs: bfloat16 [4096, 1024], P('sp', 'tp'), may hold values from -6 to 6
- log_decay: float32 [4096, 16], P('sp', 'tp'), may hold values from -1 to 0
- head_gain: float32 [1024], P('tp'), may hold values from 0.1 to 1.9
- out_weight: bfloat16 [1024, 2048], P('tp'), may hold values from -0.1875 to 0.1875
- residual: bfloat16 [4096, 2048], P(('sp', 'tp')), may hold values from -6 to 6
- norm_gain: float32 [2048], replicated, may hold values from 0.1 to 1.9
- expert_ids: int32 [4096, 2], P(('sp', 'tp')), may hold values from 0 to 15, all different within a row; in each aligned block of 128 rows (0 to 127, 128 to 255, ...) at most 32 rows name the same one
- expert_weights: float32 [4096, 2], P(('sp', 'tp')), may hold values from 0.2 to 1
- gate_experts: bfloat16 [16, 2048, 3584], P('sp', None, 'tp'), may hold values from -0.125 to 0.125
- up_experts: bfloat16 [16, 2048, 3584], P('sp', None, 'tp'), may hold values from -0.125 to 0.125
- down_experts: bfloat16 [16, 3584, 2048], P('sp', 'tp'), may hold values from -0.09375 to 0.09375
Outputs:
- layer_out: bfloat16 [4096, 2048], P(('sp', 'tp'))
The draws below stay inside these ranges and needn't reach their ends.
Inputs may be any that keep to these rules, and one draw needn't show every extreme that they name: `expert_ids`: the 2 experts of a token differ. No expert is named more than 32 times in the rows of one device, and in some device some expert is named exactly 32 times.
All inputs are finite; a program needn't handle non-finite values.
Results may differ from the reference program's by a relative error of at most 0.014.
Values may be sent and summed in bfloat16 or wider, within the bound.
A program may use at most 128 MiB of HBM per device.

```python
import math
import jax
import jax.numpy as jnp
import numpy as np
from jax import lax

D = 2048
MEMORY_CHANNELS = 16
HD = 64
FF = 3584
TOP = 2
BLOCK = 128
TOK_DEV = 256
STRING_LENGTH = 4096
EXPERTS = 16
CAP = 32
N_SP = 16
N_TP = 2


def draw_log_decay(key, part):
    concurrent_lanes = jax.random.split(key, 7)
    fast_share = 0.5
    fast = jax.random.uniform(concurrent_lanes[0], (MEMORY_CHANNELS,), jnp.float32) < fast_share
    fast_rate = jax.random.uniform(concurrent_lanes[1], (MEMORY_CHANNELS,), jnp.float32, 1.0 / 100.0, 1.0 / 30.0)
    slow_rate = jax.random.uniform(concurrent_lanes[2], (MEMORY_CHANNELS,), jnp.float32, 0.2, 0.6) / STRING_LENGTH
    reference_shrink_speed = jnp.where(fast, fast_rate, slow_rate)
    shrink_multipliers = jnp.exp(jax.random.uniform(concurrent_lanes[3], (STRING_LENGTH // BLOCK, MEMORY_CHANNELS), jnp.float32, -0.7, 0.7))
    shrink_multipliers = jnp.repeat(shrink_multipliers, BLOCK, axis=0)
    stochastic_jitter = jax.random.uniform(concurrent_lanes[4], (STRING_LENGTH, MEMORY_CHANNELS), jnp.float32, 0.5, 1.5)
    spike_occurrences = jax.random.uniform(concurrent_lanes[5], (STRING_LENGTH, MEMORY_CHANNELS), jnp.float32) < 2.0 / STRING_LENGTH
    surviving_proportion = jax.random.uniform(concurrent_lanes[6], (STRING_LENGTH, MEMORY_CHANNELS), jnp.float32, 0.5, 0.8)
    closing_result = -reference_shrink_speed[None, :] * shrink_multipliers * stochastic_jitter + jnp.where(spike_occurrences, jnp.log(surviving_proportion), 0.0)
    return closing_result.astype(jnp.float32)


def steps_of(stream_key, dims, shards, smallest, largest):
    loudness = 1.0
    for position, shards_of in shards:
        draws = jax.random.uniform(jax.random.fold_in(jax.random.fold_in(stream_key, 6), position), (shards_of,), jnp.float32, smallest / len(shards), largest / len(shards))
        loudness = loudness * jnp.repeat(jnp.exp(draws), dims[position] // shards_of).reshape((-1,) + (1,) * (len(dims) - 1 - position))
    return loudness


def assign_block(rng, own, number, rows, count, top, most, lean):
    ranking = jax.random.permutation(rng, count)
    packed, usual = portions_of(count, rows * top, most, lean, True), portions_of(count, rows * top, most, lean, False)
    places = jnp.arange(count)

    def named(sizes, rotation):
        used = int((sizes > 0).sum())
        fixed = max(1, used // 4)
        moved = fixed + (places - fixed + rotation * (used - fixed)) % max(1, count - fixed)
        return jnp.zeros((count,), jnp.int32).at[ranking[jnp.where(places < fixed, places, moved)]].set(jnp.asarray(sizes, jnp.int32))

    sizes = jnp.where(number % 4 == 0, named(packed, number // 4), named(usual, number - number // 4 - 1))
    mixed = jax.random.permutation(jax.random.fold_in(own, 3), count)
    donor, receiver = mixed[0:count // 2 * 2:2], mixed[1:count // 2 * 2:2]
    slack = jnp.minimum(sizes[donor] - 1, most - sizes[receiver]) // 2
    slack = jnp.where((donor == ranking[0]) | (receiver == ranking[0]) | (sizes[receiver] == 0), 0, jnp.maximum(slack, 0))
    moved = jax.random.randint(jax.random.fold_in(own, 4), (count // 2,), 0, 1 << 20) % (slack + 1)
    sizes = sizes.at[donor].add(-moved).at[receiver].add(moved)
    items = jnp.searchsorted(jnp.cumsum(sizes), jnp.arange(rows * top), side="right").astype(jnp.int32)
    listing = items.reshape(top, rows).T
    listing = listing[jax.random.permutation(jax.random.fold_in(own, 1), rows)]
    rotation = jax.random.randint(jax.random.fold_in(own, 2), (rows, 1), 0, top)
    return jnp.take_along_axis(listing, (jnp.arange(top)[None, :] + rotation) % top, axis=1)


def portions_of(amount, total, limit, skew, full):
    weights = [(1 << 20) // math.isqrt(grade ** skew) + 1 for grade in range(1, amount + 1)]
    largest = limit if full else min(limit, max(-(-total // amount), total * weights[0] // sum(weights)))
    least = 1 if total - largest >= amount - 1 else 0
    counts, spare = [largest] + [least] * (amount - 1), total - largest - least * (amount - 1)
    while spare > 0:
        free = [i for i in range(1, amount) if counts[i] < largest] or [i for i in range(1, amount) if counts[i] < limit]
        pool, budget = sum([weights[i] for i in free]), spare
        for i in free:
            more = min(limit - counts[i], max(1, budget * weights[i] // pool), spare)
            counts[i] = counts[i] + more
            spare = spare - more
    return np.array(counts)


def normal_values(own_key, extent, width, reach, cuts=(), kind=jnp.bfloat16):
    values = width * jax.random.normal(own_key, extent, jnp.float32)
    if cuts:
        values = values * steps_of(own_key, extent, cuts, -0.22, 0.18)
    return jnp.clip(values, -reach, reach).astype(kind)


def setup_inputs(seed: int = 0) -> dict:
    streams_of = jax.random.split(jax.random.key(seed), 15)
    queries = normal_values(streams_of[0], (STRING_LENGTH, MEMORY_CHANNELS * HD), 1.0, 6.0, ((0, 16), (1, 2)))
    key_vectors = normal_values(streams_of[1], (STRING_LENGTH, MEMORY_CHANNELS * HD), 1.0, 6.0, ((0, 16), (1, 2)))
    value_vectors = normal_values(streams_of[2], (STRING_LENGTH, MEMORY_CHANNELS * HD), 1.0, 6.0, ((0, 16), (1, 2)))
    gate_inputs = normal_values(streams_of[3], (STRING_LENGTH, MEMORY_CHANNELS * HD), 1.0, 6.0, ((0, 16), (1, 2)))
    log_decay = draw_log_decay(jax.random.fold_in(streams_of[14], 71), 0)
    head_gain = jnp.clip(1.0 + 0.18 * jax.random.normal(streams_of[5], (MEMORY_CHANNELS * HD,), jnp.float32), 0.1, 1.9)
    out_weight = normal_values(streams_of[6], (MEMORY_CHANNELS * HD, D), (MEMORY_CHANNELS * HD) ** -0.5, 0.1875, ((0, 2),))
    residual = normal_values(streams_of[7], (STRING_LENGTH, D), 1.0, 6.0, ((0, 32),))
    norm_gain = jnp.clip(1.0 + 0.18 * jax.random.normal(streams_of[8], (D,), jnp.float32), 0.1, 1.9)
    expert_ids_keys = jax.random.split(jax.random.fold_in(streams_of[9], 1), STRING_LENGTH // (TOK_DEV // N_TP))
    expert_ids_turns = jax.random.permutation(jax.random.fold_in(streams_of[9], 3), STRING_LENGTH // (TOK_DEV // N_TP))
    expert_ids = jax.vmap(lambda own, number: assign_block(jax.random.fold_in(streams_of[9], 2), own, number, TOK_DEV // N_TP, EXPERTS, TOP, CAP, 1))(expert_ids_keys, expert_ids_turns).reshape((STRING_LENGTH, TOP))
    expert_weights = jnp.clip(0.2 + 0.8 * jax.random.uniform(streams_of[10], (STRING_LENGTH, TOP), jnp.float32) ** steps_of(streams_of[10], (STRING_LENGTH, TOP), ((0, 32),), -0.2, 0.2), 0.2, 1.0)
    gate_experts = normal_values(streams_of[11], (EXPERTS, D, FF), D ** -0.5, 0.125, ((0, 16), (2, 2)))
    up_experts = normal_values(streams_of[12], (EXPERTS, D, FF), D ** -0.5, 0.125, ((0, 16), (2, 2)))
    down_experts = normal_values(streams_of[13], (EXPERTS, FF, D), FF ** -0.5, 0.09375, ((0, 16), (1, 2)))
    return dict(queries=queries, key_vectors=key_vectors, value_vectors=value_vectors, gate_inputs=gate_inputs, log_decay=log_decay, head_gain=head_gain, out_weight=out_weight, residual=residual, norm_gain=norm_gain, expert_ids=expert_ids, expert_weights=expert_weights, gate_experts=gate_experts, up_experts=up_experts, down_experts=down_experts)


def rotate(block, places):
    half_size = block.shape[-1] // 2
    frequency = 10000.0 ** (-jnp.arange(half_size, dtype=jnp.float32) / half_size)
    angles = places.astype(jnp.float32)[:, None, None] * frequency
    first_half = block[..., :half_size]
    second = block[..., half_size:]
    return jnp.concatenate([first_half * jnp.cos(angles) - second * jnp.sin(angles), second * jnp.cos(angles) + first_half * jnp.sin(angles)], axis=-1)

def to_blocks(source, blocks):
    shaped = source.reshape((blocks, source.shape[0] // blocks) + source.shape[1:])
    return jnp.swapaxes(shaped, 1, 2)

def from_blocks(source):
    shaped = jnp.swapaxes(source, 1, 2)
    return shaped.reshape((shaped.shape[0] * shaped.shape[1],) + shaped.shape[2:])

def block_step(carried_state, inputs):
    query_rows, key_rows, value_rows, decay_rows = inputs
    cumulative = jnp.cumsum(decay_rows, axis=1)
    log_gaps = cumulative[:, :, None] - cumulative[:, None, :]
    offsets = jnp.arange(decay_rows.shape[1])
    causal = offsets[:, None] >= offsets[None, :]
    decay_weight = jnp.where(causal, jnp.exp(jnp.where(causal, log_gaps, 0.0)), 0.0)
    scores = jnp.einsum('htd,hsd->hts', query_rows, key_rows, precision=lax.Precision.HIGHEST) * decay_weight
    within = jnp.einsum('hts,hse->hte', scores, value_rows, precision=lax.Precision.HIGHEST)
    carried = jnp.einsum('htd,hde->hte', query_rows * jnp.exp(cumulative)[:, :, None], carried_state, precision=lax.Precision.HIGHEST)
    last_log = cumulative[:, -1:]
    fresh_state = jnp.einsum('hsd,hse->hde', key_rows * jnp.exp(last_log - cumulative)[:, :, None], value_rows, precision=lax.Precision.HIGHEST)
    return (jnp.exp(last_log)[:, :, None] * carried_state + fresh_state, within + carried)

def round_trip(array):
    return lax.optimization_barrier(array.astype(jnp.bfloat16)).astype(jnp.float32)

def reference(queries, key_vectors, value_vectors, gate_inputs, log_decay, head_gain, out_weight, residual, norm_gain, expert_ids, expert_weights, gate_experts, up_experts, down_experts):
    places = jnp.arange(STRING_LENGTH, dtype=jnp.int32)
    turned_queries = rotate(queries.astype(jnp.float32).reshape(STRING_LENGTH, MEMORY_CHANNELS, HD), places)
    turned_keys = rotate(key_vectors.astype(jnp.float32).reshape(STRING_LENGTH, MEMORY_CHANNELS, HD), places) * HD ** (-0.5)
    value_float = value_vectors.astype(jnp.float32).reshape(STRING_LENGTH, MEMORY_CHANNELS, HD)
    blocks = STRING_LENGTH // BLOCK
    inputs = (to_blocks(turned_queries, blocks), to_blocks(turned_keys, blocks), to_blocks(value_float, blocks), to_blocks(log_decay, blocks))
    _, pieces = lax.scan(block_step, jnp.zeros((MEMORY_CHANNELS, HD, HD), jnp.float32), inputs)
    retained = from_blocks(pieces)
    squares = lax.optimization_barrier(jnp.mean(retained * retained, axis=-1, keepdims=True))
    normed = retained * lax.rsqrt(squares + 1e-06) * head_gain.reshape(MEMORY_CHANNELS, HD)
    normed = (normed.reshape(STRING_LENGTH, MEMORY_CHANNELS * HD) * jax.nn.silu(gate_inputs.astype(jnp.float32))).astype(jnp.bfloat16)
    half_heads = MEMORY_CHANNELS * HD // N_TP
    projected = jnp.zeros((STRING_LENGTH, D), jnp.float32)
    for section in range(N_TP):
        partial_value = jnp.dot(normed[:, section * half_heads:(section + 1) * half_heads], out_weight[section * half_heads:(section + 1) * half_heads], preferred_element_type=jnp.float32)
        projected = projected + round_trip(partial_value)
    mixed_rows = (residual.astype(jnp.float32) + projected).astype(jnp.bfloat16)
    mixed_float = mixed_rows.astype(jnp.float32)
    normed_rows = (mixed_float * lax.rsqrt(lax.optimization_barrier(jnp.mean(mixed_float * mixed_float, axis=-1, keepdims=True)) + 1e-06) * norm_gain).astype(jnp.bfloat16)
    sources = N_SP * N_TP
    flat_routes = expert_ids.reshape(sources, -1)
    onehot = (flat_routes[:, :, None] == jnp.arange(EXPERTS, dtype=jnp.int32)[None, None, :]).astype(jnp.int32)
    slot_rank = lax.optimization_barrier(jnp.sum(jnp.cumsum(onehot, axis=1) * onehot, axis=2)) - 1
    slot_index = (jnp.arange(sources, dtype=jnp.int32)[:, None] * CAP + slot_rank).astype(jnp.int32)
    token_index = (jnp.arange(STRING_LENGTH * TOP, dtype=jnp.int32) // TOP).reshape(sources, -1)
    table = jnp.zeros((EXPERTS, sources * CAP), jnp.int32).at[flat_routes, slot_index].set(token_index)
    slot_weight = jnp.zeros((EXPERTS, sources * CAP), expert_weights.dtype).at[flat_routes, slot_index].set(expert_weights.reshape(sources, -1))
    half_ff = FF // N_TP

    def expert_step(total, inputs):
        gate_matrix, up_matrix, down_matrix, index_rows, weight_rows = inputs
        batch = normed_rows[index_rows].astype(jnp.float32)
        gate_value = jnp.dot(batch, gate_matrix.astype(jnp.float32), precision=lax.Precision.HIGHEST)
        up_value = jnp.dot(batch, up_matrix.astype(jnp.float32), precision=lax.Precision.HIGHEST)
        hidden = round_trip(jax.nn.silu(gate_value) * up_value)
        summed = jnp.zeros((batch.shape[0], D), jnp.float32)
        for section in range(N_TP):
            partial_value = jnp.dot(hidden[:, section * half_ff:(section + 1) * half_ff], down_matrix[section * half_ff:(section + 1) * half_ff].astype(jnp.float32), precision=lax.Precision.HIGHEST)
            summed = summed + round_trip(partial_value)
        expert_out = round_trip(summed)
        return (total.at[index_rows].add(weight_rows[:, None] * expert_out), None)
    expert_sum, _ = lax.scan(expert_step, jnp.zeros((STRING_LENGTH, D), jnp.float32), (gate_experts, up_experts, down_experts, table, slot_weight))
    return (mixed_rows.astype(jnp.float32) + expert_sum).astype(jnp.bfloat16)
```

```python
import functools

import jax
import jax.numpy as jnp
from jax import lax
from jax.experimental import pallas as pl
from jax.experimental.pallas import tpu as pltpu
from jax.sharding import PartitionSpec as P

MESH = pl.DeviceIdType.MESH


def line_length(count):
    size = 1
    while size * size * size < count:
        size *= 2
    return size


def swap(value):
    return lax.ppermute(value, "tp", [(0, 1), (1, 0)])


def incoming_state(total, state):
    heads, size, _ = state.shape
    count = lax.axis_size("sp")
    state = jnp.swapaxes(state, 0, 1).reshape(size, heads * size)
    total = jnp.repeat(total, size)[None, :]

    def shift(total, state, distance):
        high = total.astype(jnp.bfloat16)
        low = (total - high.astype(jnp.float32)).astype(jnp.bfloat16)
        packed = jnp.concatenate([state.astype(jnp.bfloat16), high, low], axis=0)
        got = lax.ppermute(packed, "sp", [(i, i + distance) for i in range(count - distance)])
        got = got.astype(jnp.float32)
        return got[size : size + 1] + got[size + 1 : size + 2], got[:size]

    before_total, before_state = jnp.zeros_like(total), jnp.zeros_like(state)
    distance = 1
    while distance < count:
        earlier_total, earlier_state = shift(total, state, distance)
        before_state = jnp.exp(before_total) * earlier_state + before_state
        before_total = before_total + earlier_total
        state = jnp.exp(total) * earlier_state + state
        total = total + earlier_total
        distance *= 2
    return jnp.swapaxes(before_state.reshape(size, heads, size), 0, 1)


def rotate(block, places):
    half_size = block.shape[-1] // 2
    frequency = 10000.0 ** (-jnp.arange(half_size, dtype=jnp.float32) / half_size)
    angles = places.astype(jnp.float32)[:, None, None] * frequency
    first_half = block[..., :half_size]
    second = block[..., half_size:]
    return jnp.concatenate(
        [
            first_half * jnp.cos(angles) - second * jnp.sin(angles),
            second * jnp.cos(angles) + first_half * jnp.sin(angles),
        ],
        axis=-1,
    )


def experts_kernel(
    line,
    plane,
    cap,
    parts,
    chain,
    rows_ref,
    mixed_ref,
    meta_ref,
    gate_hbm,
    up_hbm,
    down_hbm,
    out_ref,
    gate_ref,
    up_ref,
    down_ref,
    zbuf,
    meta,
    sel,
    xbuf,
    hidden,
    ybuf,
    yin,
    sbuf,
    rbuf,
    cbuf,
    csend,
    pin,
    wsem,
    zsend,
    zrecv,
    msend,
    mrecv,
    psend,
    precv,
    tsend,
    trecv,
    ysend,
    yrecv,
    rsend,
    rrecv,
    ssend,
    srecv,
):
    sp, core = lax.axis_index("sp"), lax.axis_index("tp")
    z, p = sp // plane, lax.rem(sp, plane)
    tokens, width = rows_ref.shape
    slots = plane * cap
    f32, bf16 = jnp.float32, jnp.bfloat16

    def at(line_place, plane_place):
        return {"sp": line_place * plane + plane_place, "tp": core}

    partner = {"sp": sp, "tp": 1 - core}

    def remote(src, dst, send, recv, device):
        return pltpu.make_async_remote_copy(
            src_ref=src,
            dst_ref=dst,
            send_sem=send,
            recv_sem=recv,
            device_id=device,
            device_id_type=MESH,
        )

    weights = []
    for number, (source, target) in enumerate(
        ((gate_hbm, gate_ref), (up_hbm, up_ref), (down_hbm, down_ref))
    ):
        depth = target.shape[0] // 4
        for piece in range(4):
            part = pl.ds(piece * depth, depth)
            weights.append(
                pltpu.make_async_copy(
                    source.at[0, part], target.at[part], wsem.at[number, piece]
                )
            )

    barrier = pltpu.get_barrier_semaphore()
    peers = [at(lax.rem(z + i, line), p) for i in range(1, line)]
    peers += [at(z, lax.rem(p + i, plane)) for i in range(1, plane)] + [partner]
    for peer in peers:
        pl.semaphore_signal(barrier, inc=1, device_id=peer, device_id_type=MESH)
    for copy in weights:
        copy.start()
    pl.semaphore_wait(barrier, len(peers))

    piece_rows = tokens // parts
    chain_rows = tokens // chain

    def row_copy(way, block, part, target, source=None):
        rows = pl.ds(part * piece_rows, piece_rows)
        source = zbuf.at[block] if source is None else source
        return remote(
            source.at[rows],
            zbuf.at[block, rows],
            zsend.at[way, block, part],
            zrecv.at[block, part],
            at(target, p),
        )

    def meta_copy(i):
        return remote(
            meta_ref, meta.at[z], msend.at[i], mrecv.at[i], at(lax.rem(z + i, line), p)
        )

    for i in range(1, line):
        meta_copy(i).start()
    for part in range(parts):

        @pl.when(z + 1 < line)
        def _():
            row_copy(0, z, part, z + 1, rows_ref).start()

        @pl.when(z > 0)
        def _():
            row_copy(1, z, part, z - 1, rows_ref).start()

    meta[z] = meta_ref[...]

    near = jnp.minimum(z, line - 1 - z)
    longer_up = z < line - 1 - z

    def block_of(place):
        both = place <= 2 * near
        away = jnp.where(both, (place + 1) // 2, place - near)
        forward = jnp.where(both, place % 2 == 1, longer_up)
        return jnp.where(forward, z + away, z - away)

    def pass_on(distance):
        for part in range(parts):
            low, high = z - distance, z + distance

            @pl.when(low >= 0)
            def _():
                row_copy(0, low, part, z, rows_ref).wait_recv()

                @pl.when(z + 1 < line)
                def _():
                    row_copy(0, low, part, z + 1).start()

            @pl.when(high < line)
            def _():
                row_copy(1, high, part, z, rows_ref).wait_recv()

                @pl.when(z > 0)
                def _():
                    row_copy(1, high, part, z - 1).start()

    def slot_names():
        names = lax.broadcasted_iota(jnp.int32, (slots, tokens), 0) + z * slots
        return names.astype(f32)

    def select_copy(j, i):
        q = lax.rem(p + i, plane)
        return remote(
            sel.at[j, q], xbuf.at[j, core, p], psend.at[j, i], precv.at[j, i], at(z, q)
        )

    def select(j):
        block = block_of(j)
        names = slot_names()
        chosen = (names == meta[block, 0:1, :]) | (names == meta[block, 1:2, :])
        place = jnp.where(chosen, 1.0, 0.0).astype(bf16)
        source = rows_ref[...] if j == 0 else zbuf[block]
        picked = jnp.dot(place, source, preferred_element_type=f32)
        sel[j] = picked.reshape(plane, cap, width).astype(bf16)
        for i in range(1, plane):
            select_copy(j, i).start()
        xbuf[j, core, p] = sel[j, p]

    def partner_copy(j):
        return remote(
            xbuf.at[j, core], xbuf.at[j, core], tsend.at[j], trecv.at[j], partner
        )

    def collect(j):
        for i in range(1, plane):
            select_copy(j, i).wait_recv()
        partner_copy(j).start()

    def partial_copy(j):
        return remote(ybuf.at[j, 1 - core], yin.at[j], ysend.at[j], yrecv.at[j], partner)

    tall = 2 * slots
    wide = 256

    def multiply(j):
        partner_copy(j).wait_recv()
        if j == 0:
            for copy in weights:
                copy.wait()
        if cap % 16 == 0:
            batch = xbuf[j].reshape(tall, width)
        else:
            batch = xbuf[j].astype(f32).reshape(tall, width).astype(bf16)

        @pl.loop(0, hidden.shape[1] // wide)
        def _(tile):
            columns = pl.ds(pl.multiple_of(tile * wide, wide), wide)
            gate = jnp.dot(batch, gate_ref[:, columns], preferred_element_type=f32)
            up = jnp.dot(batch, up_ref[:, columns], preferred_element_type=f32)
            hidden[:, columns] = (gate * up / (1.0 + jnp.exp(-gate))).astype(bf16)

        @pl.loop(0, width // wide)
        def _(tile):
            columns = pl.ds(pl.multiple_of(tile * wide, wide), wide)
            value = jnp.dot(hidden[...], down_ref[:, columns], preferred_element_type=f32)
            ybuf[j, :, :, :, columns] = value.reshape(2, plane, cap, wide).astype(bf16)

        partial_copy(j).start()

    def return_copy(j, i):
        q = lax.rem(p + i, plane)
        return remote(
            sbuf.at[j, q], rbuf.at[j, p], rsend.at[j, i], rrecv.at[j, i], at(z, q)
        )

    def give_back(j):
        partial_copy(j).wait_recv()
        sbuf[j] = (ybuf[j, core].astype(f32) + yin[j].astype(f32)).astype(bf16)
        for i in range(1, plane):
            return_copy(j, i).start()
        rbuf[j, p] = sbuf[j, p]

    def chain_copy(way, block, part, target):
        rows = pl.ds(part * chain_rows, chain_rows)
        return remote(
            csend.at[block, rows],
            pin.at[way, block, rows],
            ssend.at[block, part],
            srecv.at[way, block, part],
            at(target, p),
        )

    def combine(j):
        for i in range(1, plane):
            return_copy(j, i).wait_recv()
        block = block_of(j)
        names = slot_names()
        weigh = jnp.where(names == meta[block, 0:1, :], meta[block, 2:3, :], 0.0)
        weigh = weigh + jnp.where(names == meta[block, 1:2, :], meta[block, 3:4, :], 0.0)
        weigh = weigh.T
        high = weigh.astype(bf16)
        low = (weigh - high.astype(f32)).astype(bf16)
        if cap % 16 == 0:
            back = rbuf[j].reshape(slots, width)
        else:
            back = rbuf[j].astype(f32).reshape(slots, width).astype(bf16)
        total = jnp.dot(high, back, preferred_element_type=f32) + jnp.dot(
            low, back, preferred_element_type=f32
        )
        if j == 0:
            cbuf[block] = total + mixed_ref[...].astype(f32)
        else:
            cbuf[block] = total

            @pl.when((z == 0) | (z == line - 1))
            def _():
                csend[block] = total.astype(bf16)

            for part in range(chain):

                @pl.when(z == 0)
                def _():
                    chain_copy(0, block, part, z + 1).start()

                @pl.when(z == line - 1)
                def _():
                    chain_copy(1, block, part, z - 1).start()

    select(0)
    collect(0)
    for i in range(1, line):
        meta_copy(i).wait_recv()
    for j in range(line):
        if j + 1 < line:
            pass_on(j + 1)
            select(j + 1)
        multiply(j)
        if j + 1 < line:
            collect(j + 1)
        if j >= 1:
            combine(j - 1)
        give_back(j)
    combine(line - 1)

    def relay(way, block, last, step):
        inside = (z < block) & (z > 0) if way == 0 else (z > block) & (z < line - 1)
        fed = z > 0 if way == 0 else z < line - 1
        for part in range(chain):
            rows = pl.ds(part * chain_rows, chain_rows)

            @pl.when(inside)
            def _():
                chain_copy(way, block, part, z).wait_recv()
                total = cbuf[block, rows] + pin[way, block, rows].astype(f32)
                csend[block, rows] = total.astype(bf16)
                chain_copy(way, block, part, z + step).start()

            @pl.when(fed & (z == block))
            def _():
                chain_copy(way, block, part, z).wait_recv()
                cbuf[block, rows] = cbuf[block, rows] + pin[way, block, rows].astype(f32)

    for i in range(1, line):
        relay(0, i, line - 1, 1)
        relay(1, line - 1 - i, 0, -1)
    out_ref[...] = cbuf[z].astype(bf16)

    for i in range(1, line):
        meta_copy(i).wait_send()
    for part in range(parts):
        for block in range(line):

            @pl.when((z >= block) & (z + 1 < line))
            def _():
                row_copy(0, block, part, z, rows_ref).wait_send()

            @pl.when((z <= block) & (z > 0))
            def _():
                row_copy(1, block, part, z, rows_ref).wait_send()

    for part in range(chain):
        for block in range(line):

            @pl.when(z != block)
            def _():
                chain_copy(0, block, part, z).wait_send()

    for j in range(line):
        for i in range(1, plane):
            select_copy(j, i).wait_send()
            return_copy(j, i).wait_send()
        partner_copy(j).wait_send()
        partial_copy(j).wait_send()


def run_experts(rows, mixed, meta, gate, up, down, cap):
    count = lax.axis_size("sp")
    line = line_length(count)
    plane = count // line
    tokens, width = rows.shape
    inner = gate.shape[2]
    slots = plane * cap
    parts, chain = 2, 4
    bf16, f32 = jnp.bfloat16, jnp.float32
    dma = pltpu.SemaphoreType.DMA
    vmem = pl.BlockSpec(memory_space=pltpu.VMEM)
    hbm = pl.BlockSpec(memory_space=pl.ANY)
    return pl.pallas_call(
        functools.partial(experts_kernel, line, plane, cap, parts, chain),
        out_shape=jax.ShapeDtypeStruct((tokens, width), bf16),
        in_specs=[vmem] * 3 + [hbm] * 3,
        out_specs=vmem,
        scratch_shapes=[
            pltpu.VMEM((width, inner), bf16),
            pltpu.VMEM((width, inner), bf16),
            pltpu.VMEM((inner, width), bf16),
            pltpu.VMEM((line, tokens, width), bf16),
            pltpu.VMEM((line,) + meta.shape, f32),
            pltpu.VMEM((line, plane, cap, width), bf16),
            pltpu.VMEM((line, 2, plane, cap, width), bf16),
            pltpu.VMEM((2 * slots, inner), bf16),
            pltpu.VMEM((line, 2, plane, cap, width), bf16),
            pltpu.VMEM((line, plane, cap, width), bf16),
            pltpu.VMEM((line, plane, cap, width), bf16),
            pltpu.VMEM((line, plane, cap, width), bf16),
            pltpu.VMEM((line, tokens, width), f32),
            pltpu.VMEM((line, tokens, width), bf16),
            pltpu.VMEM((2, line, tokens, width), bf16),
            dma((3, 4)),
            dma((2, line, parts)),
            dma((line, parts)),
            dma((line,)),
            dma((line,)),
            dma((line, plane)),
            dma((line, plane)),
            dma((line,)),
            dma((line,)),
            dma((line,)),
            dma((line,)),
            dma((line, plane)),
            dma((line, plane)),
            dma((line, chain)),
            dma((2, line, chain)),
        ],
        compiler_params=pltpu.CompilerParams(
            collective_id=1, has_side_effects=True, vmem_limit_bytes=62 * 1024 * 1024
        ),
        name="experts",
    )(rows, mixed, meta, gate, up, down)


def shards(
    queries,
    key_vectors,
    value_vectors,
    gate_inputs,
    log_decay,
    head_gain,
    out_weight,
    residual,
    norm_gain,
    expert_ids,
    expert_weights,
    gate_experts,
    up_experts,
    down_experts,
):
    tok_dev, channels = queries.shape
    head_count = log_decay.shape[1]
    head_size = channels // head_count
    places = lax.axis_index("sp") * tok_dev + jnp.arange(tok_dev, dtype=jnp.int32)
    core = lax.axis_index("tp")
    turned_queries = rotate(
        queries.astype(jnp.float32).reshape(tok_dev, head_count, head_size), places
    )
    turned_keys = rotate(
        key_vectors.astype(jnp.float32).reshape(tok_dev, head_count, head_size), places
    ) * head_size ** (-0.5)
    value_float = value_vectors.astype(jnp.float32).reshape(tok_dev, head_count, head_size)
    running = jnp.cumsum(log_decay, axis=0)
    device_total = running[-1]
    end_weight = jnp.exp(device_total[None, :] - running)
    local_end = jnp.einsum(
        "thd,the->hde",
        turned_keys * end_weight[:, :, None],
        value_float,
        precision=lax.Precision.HIGH,
    )
    incoming = incoming_state(device_total, local_end)
    by_head = running.T
    log_gaps = by_head[:, :, None] - by_head[:, None, :]
    offsets = jnp.arange(tok_dev)
    causal = offsets[:, None] >= offsets[None, :]
    decay_weight = jnp.where(causal, jnp.exp(jnp.where(causal, log_gaps, 0.0)), 0.0)
    scores = (
        jnp.einsum("thd,shd->hts", turned_queries, turned_keys, precision=lax.Precision.HIGH)
        * decay_weight
    )
    within = jnp.einsum("hts,she->the", scores, value_float, precision=lax.Precision.HIGH)
    carried = jnp.einsum(
        "thd,hde->the",
        turned_queries * jnp.exp(running)[:, :, None],
        incoming,
        precision=lax.Precision.HIGH,
    )
    retained = within + carried
    squares = jnp.mean(retained * retained, axis=-1, keepdims=True)
    normed = retained * lax.rsqrt(squares + 1e-06) * head_gain.reshape(head_count, head_size)
    normed = (
        normed.reshape(tok_dev, channels) * jax.nn.silu(gate_inputs.astype(jnp.float32))
    ).astype(jnp.bfloat16)
    half = tok_dev // 2
    normed_away = lax.dynamic_slice_in_dim(normed, (1 - core) * half, half, 0)
    normed_here = lax.dynamic_slice_in_dim(normed, core * half, half, 0)
    away = jnp.dot(normed_away, out_weight, preferred_element_type=jnp.float32)
    got = swap(away.astype(jnp.bfloat16))
    here = jnp.dot(normed_here, out_weight, preferred_element_type=jnp.float32)
    projected = here.astype(jnp.bfloat16).astype(jnp.float32) + got.astype(jnp.float32)
    mixed_rows = (residual.astype(jnp.float32) + projected).astype(jnp.bfloat16)
    mixed_float = mixed_rows.astype(jnp.float32)
    normed_rows = (
        mixed_float
        * lax.rsqrt(jnp.mean(mixed_float * mixed_float, axis=-1, keepdims=True) + 1e-06)
        * norm_gain
    ).astype(jnp.bfloat16)
    experts = lax.axis_size("sp")
    capacity = 2 * tok_dev // experts
    top_count = expert_ids.shape[1]
    flat_routes = expert_ids.reshape(-1)
    onehot = (flat_routes[:, None] == jnp.arange(experts, dtype=jnp.int32)[None, :]).astype(
        jnp.int32
    )
    slot_rank = jnp.sum(jnp.cumsum(onehot, axis=0) * onehot, axis=1) - 1
    slot = (flat_routes * capacity + slot_rank).reshape(-1, top_count)
    meta = jnp.concatenate(
        [
            slot.T.astype(jnp.float32),
            expert_weights.T,
            jnp.zeros((8 - 2 * top_count, half), jnp.float32),
        ],
        axis=0,
    )
    return run_experts(
        normed_rows, mixed_rows, meta, gate_experts, up_experts, down_experts, capacity
    )


def solution(mesh):
    return jax.shard_map(
        shards,
        mesh=mesh,
        in_specs=(
            P("sp", "tp"),
            P("sp", "tp"),
            P("sp", "tp"),
            P("sp", "tp"),
            P("sp", "tp"),
            P("tp"),
            P("tp", None),
            P(("sp", "tp"), None),
            P(),
            P(("sp", "tp"), None),
            P(("sp", "tp"), None),
            P("sp", None, "tp"),
            P("sp", None, "tp"),
            P("sp", "tp", None),
        ),
        out_specs=P(("sp", "tp"), None),
        check_vma=False,
    )
```

```python
import functools

import jax
import jax.numpy as jnp
from jax import lax
from jax.experimental import pallas as pl
from jax.experimental.pallas import tpu as pltpu
from jax.sharding import PartitionSpec as P

MESH = pl.DeviceIdType.MESH


def line_length(count):
    size = 1
    while size * size * size < count:
        size *= 2
    return size


def layer_kernel(
    line,
    plane,
    cap,
    parts,
    halves,
    chain,
    query_hbm,
    key_hbm,
    value_hbm,
    gates_hbm,
    decay_ref,
    gain_ref,
    project_hbm,
    residual_hbm,
    norm_ref,
    route_ref,
    cos_ref,
    sin_ref,
    gate_hbm,
    up_hbm,
    down_hbm,
    out_ref,
    query_ref,
    key_ref,
    value_ref,
    gates_ref,
    project_ref,
    residual_ref,
    running_ref,
    by_head_ref,
    turned_query,
    turned_key,
    start_query,
    within_ref,
    normed_ref,
    away_ref,
    got_ref,
    mixed_ref,
    meta_ref,
    state_out,
    state_in,
    totals,
    before_ref,
    plane_state,
    plane_total,
    line_state,
    line_total,
    carry_ref,
    back_state,
    start_state,
    lsem,
    asend,
    arecv,
    bsend,
    brecv,
    ctsend,
    ctrecv,
    dsend,
    drecv,
    esend,
    erecv,
    gate_ref,
    up_ref,
    down_ref,
    zbuf,
    meta,
    sel,
    xbuf,
    hidden,
    ybuf,
    yin,
    sbuf,
    rbuf,
    cbuf,
    csend,
    pin,
    wsem,
    zsend,
    zrecv,
    msend,
    mrecv,
    psend,
    precv,
    tsend,
    trecv,
    ysend,
    yrecv,
    rsend,
    rrecv,
    ssend,
    srecv,
):
    sp, core = lax.axis_index("sp"), lax.axis_index("tp")
    z, p = sp // plane, lax.rem(sp, plane)
    length, channels = query_ref.shape
    tokens, width = residual_ref.shape
    lanes = cos_ref.shape[1]
    heads = decay_ref.shape[1]
    size = channels // heads
    pack = lanes // size
    groups = channels // lanes
    slice_rows = state_out.shape[1]
    slots = plane * cap
    f32, bf16 = jnp.float32, jnp.bfloat16

    def at(line_place, plane_place):
        return {"sp": line_place * plane + plane_place, "tp": core}

    partner = {"sp": sp, "tp": 1 - core}

    def remote(src, dst, send, recv, device):
        return pltpu.make_async_remote_copy(
            src_ref=src,
            dst_ref=dst,
            send_sem=send,
            recv_sem=recv,
            device_id=device,
            device_id_type=MESH,
        )

    loads = [
        pltpu.make_async_copy(source, target, lsem.at[number])
        for number, (source, target) in enumerate(
            (
                (query_hbm, query_ref),
                (key_hbm, key_ref),
                (value_hbm, value_ref),
                (gates_hbm, gates_ref),
                (project_hbm, project_ref),
                (residual_hbm, residual_ref),
            )
        )
    ]
    for copy in loads:
        copy.start()

    weights = []
    for number, (source, target) in enumerate(
        ((gate_hbm, gate_ref), (up_hbm, up_ref), (down_hbm, down_ref))
    ):
        depth = target.shape[0] // 4
        for piece in range(4):
            part = pl.ds(piece * depth, depth)
            weights.append(
                pltpu.make_async_copy(
                    source.at[0, part], target.at[part], wsem.at[number, piece]
                )
            )

    barrier = pltpu.get_barrier_semaphore()
    peers = [at(lax.rem(z + i, line), p) for i in range(1, line)]
    peers += [at(z, lax.rem(p + i, plane)) for i in range(1, plane)] + [partner]
    for peer in peers:
        pl.semaphore_signal(barrier, inc=1, device_id=peer, device_id_type=MESH)
    for copy in weights:
        copy.start()

    lane = lax.broadcasted_iota(jnp.int32, (1, lanes), 1)
    contract = (((1,), (1,)), ((), ()))
    upright = (((0,), (0,)), ((), ()))

    def place_of(group):
        return pl.ds(pl.multiple_of(group * lanes, lanes), lanes)

    def by_lane(pieces):
        value = pieces[-1]
        for number in range(pack - 2, -1, -1):
            value = jnp.where(lane < (number + 1) * size, pieces[number], value)
        return value

    count = line * plane
    expert = lax.broadcasted_iota(jnp.int32, (count, tokens), 0).astype(f32)
    first_hot = jnp.where(expert == route_ref[0:1, :], 1.0, 0.0)
    second_hot = jnp.where(expert == route_ref[1:2, :], 1.0, 0.0)
    earlier = lax.broadcasted_iota(jnp.int32, (tokens, tokens), 0) < (
        lax.broadcasted_iota(jnp.int32, (tokens, tokens), 1)
    )
    taken = jnp.dot(
        (first_hot + second_hot).astype(bf16),
        jnp.where(earlier, 1.0, 0.0).astype(bf16),
        preferred_element_type=f32,
    )
    first_rank = jnp.sum(first_hot * taken, axis=0, keepdims=True)
    second_rank = jnp.sum(second_hot * taken, axis=0, keepdims=True)
    meta_ref[...] = route_ref[...]
    meta_ref[0:1, :] = route_ref[0:1, :] * cap + first_rank
    meta_ref[1:2, :] = route_ref[1:2, :] * cap + second_rank

    rows_of = lax.broadcasted_iota(jnp.int32, (length, length), 0)
    columns_of = lax.broadcasted_iota(jnp.int32, (length, length), 1)
    causal = rows_of >= columns_of
    lower = jnp.where(causal, 1.0, 0.0).astype(bf16)
    upper = jnp.where(rows_of <= columns_of, 1.0, 0.0).astype(bf16)
    spread = lax.broadcasted_iota(jnp.int32, (heads, channels), 1) // size == (
        lax.broadcasted_iota(jnp.int32, (heads, channels), 0)
    )
    spread = jnp.where(spread, 1.0, 0.0).astype(bf16)
    rest = decay_ref[...]
    running, by_head = 0.0, 0.0
    for _ in range(3):
        piece = rest.astype(bf16)
        rest = rest - piece.astype(f32)
        wide_piece = jnp.dot(piece, spread, preferred_element_type=f32).astype(bf16)
        running = running + jnp.dot(lower, wide_piece, preferred_element_type=f32)
        by_head = by_head + lax.dot_general(piece, upper, upright, preferred_element_type=f32)
    running_ref[...] = running
    by_head_ref[...] = by_head

    swapped = lax.broadcasted_iota(jnp.int32, (lanes, lanes), 0) == (
        lax.broadcasted_iota(jnp.int32, (lanes, lanes), 1) ^ (size // 2)
    )
    swapped = jnp.where(swapped, 1.0, 0.0).astype(bf16)
    for copy in loads[:3]:
        copy.wait()

    def turn(block):
        other = jnp.dot(block, swapped, preferred_element_type=f32)
        return block.astype(f32) * cos_ref[...] + other * sin_ref[...]

    for group in range(groups):
        where = pl.ds(group * lanes, lanes)
        run = running_ref[:, where]
        query = turn(query_ref[:, where])
        key = turn(key_ref[:, where]) * size ** (-0.5)
        turned_query[:, where] = query.astype(bf16)
        turned_key[:, where] = key.astype(bf16)
        start_query[:, where] = (query * jnp.exp(run)).astype(bf16)
        end = run[length - 1 : length, :]
        final = lax.dot_general(
            (key * jnp.exp(end - run)).astype(bf16),
            value_ref[:, where],
            upright,
            preferred_element_type=f32,
        )
        state = by_lane([final[n * size : (n + 1) * size, :] for n in range(pack)])
        totals[p, group] = jnp.broadcast_to(end, totals.shape[2:])
        per = size // slice_rows if slice_rows < size else 1
        deep = min(slice_rows, size)
        for part in range(per):
            row = group * size + part * deep
            state_out[row // slice_rows, pl.ds(row % slice_rows, deep), :] = state[
                part * deep : (part + 1) * deep, :
            ].astype(bf16)
    state_in[p] = state_out[p]

    pl.semaphore_wait(barrier, len(peers))

    def state_copy(i):
        q = lax.rem(p + i, plane)
        return remote(
            state_out.at[q], state_in.at[p], asend.at[i], arecv.at[i], at(z, q)
        )

    def total_copy(i):
        q = lax.rem(p + i, plane)
        return remote(totals.at[p], totals.at[p], bsend.at[i], brecv.at[i], at(z, q))

    for i in range(1, plane):
        state_copy(i).start()
        total_copy(i).start()

    def meta_copy(i):
        return remote(
            meta_ref, meta.at[z], msend.at[i], mrecv.at[i], at(lax.rem(z + i, line), p)
        )

    for i in range(1, line):
        meta_copy(i).start()

    def attend(lo, hi):
        @pl.loop(lo, hi)
        def _(group):
            where = place_of(group)
            query, key, value = turned_query[:, where], turned_key[:, where], value_ref[:, where]
            run = running_ref[:, where]
            total = []
            for number in range(pack):
                mine = (lane >= number * size) & (lane < (number + 1) * size)
                masked = jnp.where(mine, query, jnp.zeros_like(query))
                score = lax.dot_general(masked, key, contract, preferred_element_type=f32)
                gap = run[:, number * size : number * size + 1] - by_head_ref[
                    pl.ds(group * pack + number, 1), :
                ]
                ok = lax.broadcasted_iota(jnp.int32, (length, length), 0) >= (
                    lax.broadcasted_iota(jnp.int32, (length, length), 1)
                )
                weight = jnp.where(ok, jnp.exp(jnp.where(ok, gap, 0.0)), 0.0)
                total.append(
                    jnp.dot((score * weight).astype(bf16), value, preferred_element_type=f32)
                )
            within_ref[:, where] = by_lane(total)

    attend(0, groups // 2)

    mine = p * slice_rows // size
    for i in range(1, plane):
        state_copy(i).wait_recv()
        total_copy(i).wait_recv()
    held = jnp.zeros((slice_rows, lanes), f32)
    elapsed = jnp.zeros((1, lanes), f32)
    for q in range(plane):
        before_ref[q] = held
        step = totals[q, mine][0:1, :]
        held = jnp.exp(step) * held + state_in[q].astype(f32)
        elapsed = elapsed + step
    plane_state[...] = held.astype(bf16)
    plane_total[...] = jnp.broadcast_to(elapsed, plane_total.shape)

    def line_state_copy(i):
        return remote(
            plane_state, line_state.at[z], ctsend.at[i, 0], ctrecv.at[i, 0], at(z + i, p)
        )

    def line_total_copy(i):
        return remote(
            plane_total, line_total.at[z], ctsend.at[i, 1], ctrecv.at[i, 1], at(z + i, p)
        )

    for i in range(1, line):

        @pl.when(z + i < line)
        def _():
            line_state_copy(i).start()
            line_total_copy(i).start()

    attend(groups // 2, groups)

    carry_ref[...] = jnp.zeros_like(carry_ref)
    for i in range(line - 1, 0, -1):

        @pl.when(z >= i)
        def _():
            line_state_copy(i).wait_recv()
            line_total_copy(i).wait_recv()
            step = line_total[z - i][0:1, :]
            carry_ref[...] = jnp.exp(step) * carry_ref[...] + line_state[z - i].astype(f32)

    elapsed = jnp.zeros((1, lanes), f32)
    for q in range(plane):
        value = before_ref[q] + jnp.exp(elapsed) * carry_ref[...]
        back_state[q] = value.astype(bf16)
        elapsed = elapsed + totals[q, mine][0:1, :]

    def start_copy(i):
        q = lax.rem(p + i, plane)
        return remote(
            back_state.at[q], start_state.at[p], dsend.at[i], drecv.at[i], at(z, q)
        )

    for i in range(1, plane):
        start_copy(i).start()
    start_state[p] = back_state[p]
    for copy in loads[3:]:
        copy.wait()
    for i in range(1, plane):
        start_copy(i).wait_recv()

    for group in range(groups):
        where = pl.ds(group * lanes, lanes)
        pieces = []
        for part in range(max(1, size // slice_rows)):
            row = group * size + part * slice_rows
            deep = min(slice_rows, size)
            pieces.append(start_state[row // slice_rows, pl.ds(row % slice_rows, deep), :])
        state = pieces[0] if len(pieces) == 1 else jnp.concatenate(pieces, axis=0)
        diagonal = jnp.concatenate(
            [
                jnp.where(
                    (lane >= n * size) & (lane < (n + 1) * size), state, jnp.zeros_like(state)
                )
                for n in range(pack)
            ],
            axis=0,
        )
        retained = within_ref[:, where] + jnp.dot(
            start_query[:, where], diagonal, preferred_element_type=f32
        )
        square = retained * retained
        sums = [
            jnp.sum(
                jnp.where((lane >= n * size) & (lane < (n + 1) * size), square, 0.0),
                axis=1,
                keepdims=True,
            )
            for n in range(pack)
        ]
        mean = by_lane(sums) * (1.0 / size)
        gates = gates_ref[:, where].astype(f32)
        normed = retained * lax.rsqrt(mean + 1e-06) * gain_ref[:, where]
        normed = normed * (gates / (1.0 + jnp.exp(-gates)))
        normed_ref[:, where] = normed.astype(bf16)

    def away_copy(h):
        columns = pl.ds(h * (width // 2), width // 2)
        return remote(
            away_ref.at[:, columns], got_ref.at[:, columns], esend.at[h], erecv.at[h], partner
        )

    away_rows = pl.ds(pl.multiple_of((1 - core) * tokens, tokens), tokens)
    here_rows = pl.ds(pl.multiple_of(core * tokens, tokens), tokens)
    for h in range(2):
        columns = pl.ds(h * (width // 2), width // 2)
        away_ref[:, columns] = jnp.dot(
            normed_ref[away_rows, :], project_ref[:, columns], preferred_element_type=f32
        ).astype(bf16)
        away_copy(h).start()
    squares = jnp.zeros((tokens, 1), f32)
    for h in range(2):
        columns = pl.ds(h * (width // 2), width // 2)
        here = jnp.dot(
            normed_ref[here_rows, :], project_ref[:, columns], preferred_element_type=f32
        ).astype(bf16)
        away_copy(h).wait_recv()
        projected = here.astype(f32) + got_ref[:, columns].astype(f32)
        mixed = (residual_ref[:, columns].astype(f32) + projected).astype(bf16)
        mixed_ref[:, columns] = mixed
        mixed = mixed.astype(f32)
        squares = squares + jnp.sum(mixed * mixed, axis=1, keepdims=True)
    scale = lax.rsqrt(squares * (1.0 / width) + 1e-06)
    for h in range(2):
        columns = pl.ds(h * (width // 2), width // 2)
        normed = mixed_ref[:, columns].astype(f32) * scale * norm_ref[:, columns]
        zbuf[z, :, columns] = normed.astype(bf16)

    piece_rows = tokens // parts
    chain_width = width // chain

    def row_copy(way, block, part, target):
        rows = pl.ds(part * piece_rows, piece_rows)
        return remote(
            zbuf.at[block, rows],
            zbuf.at[block, rows],
            zsend.at[way, block, part],
            zrecv.at[block, part],
            at(target, p),
        )

    for part in range(parts):

        @pl.when(z + 1 < line)
        def _():
            row_copy(0, z, part, z + 1).start()

        @pl.when(z > 0)
        def _():
            row_copy(1, z, part, z - 1).start()

    meta[z] = meta_ref[...]

    near = jnp.minimum(z, line - 1 - z)
    longer_up = z < line - 1 - z

    def block_of(place):
        both = place <= 2 * near
        away = jnp.where(both, (place + 1) // 2, place - near)
        forward = jnp.where(both, place % 2 == 1, longer_up)
        return jnp.where(forward, z + away, z - away)

    def pass_on(distance, lo, hi):
        for part in range(lo, hi):
            low, high = z - distance, z + distance

            @pl.when(low >= 0)
            def _():
                row_copy(0, low, part, z).wait_recv()

                @pl.when(z + 1 < line)
                def _():
                    row_copy(0, low, part, z + 1).start()

            @pl.when(high < line)
            def _():
                row_copy(1, high, part, z).wait_recv()

                @pl.when(z > 0)
                def _():
                    row_copy(1, high, part, z - 1).start()

    def slot_names():
        names = lax.broadcasted_iota(jnp.int32, (slots, tokens), 0) + z * slots
        return names.astype(f32)

    def select_copy(j, i):
        q = lax.rem(p + i, plane)
        return remote(
            sel.at[j, q], xbuf.at[j, core, p], psend.at[j, i], precv.at[j, i], at(z, q)
        )

    def select(j):
        block = block_of(j)
        names = slot_names()
        chosen = (names == meta[block, 0:1, :]) | (names == meta[block, 1:2, :])
        place = jnp.where(chosen, 1.0, 0.0).astype(bf16)
        picked = jnp.dot(place, zbuf[block], preferred_element_type=f32)
        sel[j] = picked.reshape(plane, cap, width).astype(bf16)
        for i in range(1, plane):
            select_copy(j, i).start()
        xbuf[j, core, p] = sel[j, p]

    def partner_copy(j):
        return remote(
            xbuf.at[j, core], xbuf.at[j, core], tsend.at[j], trecv.at[j], partner
        )

    def collect(j):
        for i in range(1, plane):
            select_copy(j, i).wait_recv()
        partner_copy(j).start()

    half = width // halves

    def partial_copy(j, h):
        columns = pl.ds(h * half, half)
        return remote(
            ybuf.at[j, 1 - core, :, :, columns],
            yin.at[j, :, :, columns],
            ysend.at[j, h],
            yrecv.at[j, h],
            partner,
        )

    tall = 2 * slots
    wide = 256

    def widen(j, lo, hi):
        if lo == hi:
            return
        if cap % 16 == 0:
            batch = xbuf[j].reshape(tall, width)
        else:
            batch = xbuf[j].astype(f32).reshape(tall, width).astype(bf16)

        @pl.loop(lo, hi)
        def _(tile):
            columns = pl.ds(pl.multiple_of(tile * wide, wide), wide)
            gate = jnp.dot(batch, gate_ref[:, columns], preferred_element_type=f32)
            up = jnp.dot(batch, up_ref[:, columns], preferred_element_type=f32)
            hidden[:, columns] = (gate * up / (1.0 + jnp.exp(-gate))).astype(bf16)

    def narrow(j, h):
        @pl.loop(h * (half // wide), (h + 1) * (half // wide))
        def _(tile):
            columns = pl.ds(pl.multiple_of(tile * wide, wide), wide)
            value = jnp.dot(hidden[...], down_ref[:, columns], preferred_element_type=f32)
            ybuf[j, :, :, :, columns] = value.reshape(2, plane, cap, wide).astype(bf16)

        partial_copy(j, h).start()

    def return_copy(j, i, h):
        q = lax.rem(p + i, plane)
        columns = pl.ds(h * half, half)
        return remote(
            sbuf.at[j, q, :, columns],
            rbuf.at[j, p, :, columns],
            rsend.at[j, i, h],
            rrecv.at[j, i, h],
            at(z, q),
        )

    def give_back(j, h):
        columns = pl.ds(h * half, half)
        partial_copy(j, h).wait_recv()
        total = ybuf[j, core, :, :, columns].astype(f32) + yin[j, :, :, columns].astype(f32)
        sbuf[j, :, :, columns] = total.astype(bf16)
        for i in range(1, plane):
            return_copy(j, i, h).start()
        rbuf[j, p, :, columns] = sbuf[j, p, :, columns]

    def chain_copy(way, block, part, target):
        columns = pl.ds(part * chain_width, chain_width)
        return remote(
            csend.at[block, :, columns],
            pin.at[way, block, :, columns],
            ssend.at[block, part],
            srecv.at[way, block, part],
            at(target, p),
        )

    def weigh_of(j):
        block = block_of(j)
        names = slot_names()
        weigh = jnp.where(names == meta[block, 0:1, :], meta[block, 2:3, :], 0.0)
        weigh = weigh + jnp.where(names == meta[block, 1:2, :], meta[block, 3:4, :], 0.0)
        weigh = weigh.T
        high = weigh.astype(bf16)
        return high, (weigh - high.astype(f32)).astype(bf16)

    def combine(j, h, weigh):
        for i in range(1, plane):
            return_copy(j, i, h).wait_recv()
        block = block_of(j)
        high, low = weigh
        columns = pl.ds(h * half, half)
        if cap % 16 == 0:
            back = rbuf[j, :, :, columns].reshape(slots, half)
        else:
            back = rbuf[j, :, :, columns].astype(f32).reshape(slots, half).astype(bf16)
        total = jnp.dot(high, back, preferred_element_type=f32) + jnp.dot(
            low, back, preferred_element_type=f32
        )
        if j == 0:
            cbuf[block, :, columns] = total + mixed_ref[:, columns].astype(f32)
        else:
            cbuf[block, :, columns] = total

            @pl.when((z == 0) | (z == line - 1))
            def _():
                csend[block, :, columns] = total.astype(bf16)

            for part in range(h * chain // halves, (h + 1) * chain // halves):

                @pl.when(z == 0)
                def _():
                    chain_copy(0, block, part, z + 1).start()

                @pl.when(z == line - 1)
                def _():
                    chain_copy(1, block, part, z - 1).start()

    def relay(way, block, part):
        before = jnp.where(way == 0, z < block, z > block)
        inside = before & (z > 0) & (z < line - 1)
        columns = pl.ds(part * chain_width, chain_width)

        @pl.when(inside)
        def _():
            chain_copy(way, block, part, z).wait_recv()
            total = cbuf[block, :, columns] + pin[way, block, :, columns].astype(f32)
            csend[block, :, columns] = total.astype(bf16)
            chain_copy(way, block, part, z + 1 - 2 * way).start()

    first_way = jnp.where(2 * z < line, 0, 1)

    def relays(i, lo, hi):
        def one(way, part):
            relay(way, jnp.where(way == 0, i, line - 1 - i), part)

        for part in range(lo, hi + lag):
            if part < hi:
                one(first_way, part)
            if part >= lo + lag:
                one(1 - first_way, part - lag)

    lag = chain // 2
    tiles = hidden.shape[1] // wide
    sc = jax.named_scope
    with sc("select#0"):
        select(0)
    with sc("meta"):
        for i in range(1, line):
            meta_copy(i).wait_recv()
    with sc("pass#1a"):
        pass_on(1, 0, parts // 2)
    with sc("collect#0"):
        collect(0)
    for j in range(line):
        last = j + 1 == line
        cut = max(0, tiles - j * tiles // 2)
        with sc(f"xwait#{j}"):
            partner_copy(j).wait_recv()
            if j == 0:
                for copy in weights:
                    copy.wait()
        with sc(f"widen#{j}a"):
            widen(j, 0, cut)
        if not last:
            with sc(f"pass#{j + 1}b"):
                pass_on(j + 1, parts // 2, parts)
            with sc(f"select#{j + 1}"):
                select(j + 1)
        with sc(f"widen#{j}b"):
            widen(j, cut, tiles)
        if j >= 1:
            with sc(f"combine#{j - 1}"):
                weigh = weigh_of(j - 1)
                for h in range(halves):
                    combine(j - 1, h, weigh)
        with sc(f"narrow#{j}a"):
            narrow(j, 0)
        with sc(f"narrow#{j}b"):
            for h in range(1, halves):
                narrow(j, h)
        if j + 2 < line:
            with sc(f"pass#{j + 2}a"):
                pass_on(j + 2, 0, parts // 2)
        if not last:
            with sc(f"collect#{j + 1}"):
                collect(j + 1)
        with sc(f"give#{j}"):
            for h in range(halves):
                give_back(j, h)
        if 2 <= j < line - 2:
            relays(j, 0, chain)
    weigh = weigh_of(line - 1)
    share = chain // halves
    for h in range(halves):
        if line > 2:
            with sc(f"relays#a{h}"):
                relays(line - 2, h * share, h * share + share // 2)
        with sc(f"combine#last{h}"):
            combine(line - 1, h, weigh)
        if line > 2:
            with sc(f"relays#b{h}"):
                relays(line - 2, h * share + share // 2, (h + 1) * share)
    with sc("relays#c"):
        relays(line - 1, 0, chain)
    with sc("own"):
        for part in range(chain):
            columns = pl.ds(part * chain_width, chain_width)

            @pl.when(z > 0)
            def _():
                chain_copy(0, z, part, z).wait_recv()
                cbuf[z, :, columns] = cbuf[z, :, columns] + pin[0, z, :, columns].astype(f32)

            @pl.when(z < line - 1)
            def _():
                chain_copy(1, z, part, z).wait_recv()
                cbuf[z, :, columns] = cbuf[z, :, columns] + pin[1, z, :, columns].astype(f32)

    out_ref[...] = cbuf[z].astype(bf16)

    for i in range(1, line):
        meta_copy(i).wait_send()

        @pl.when(z + i < line)
        def _():
            line_state_copy(i).wait_send()
            line_total_copy(i).wait_send()

    for i in range(1, plane):
        state_copy(i).wait_send()
        total_copy(i).wait_send()
        start_copy(i).wait_send()
    for h in range(2):
        away_copy(h).wait_send()
    for part in range(parts):
        for block in range(line):

            @pl.when((z >= block) & (z + 1 < line))
            def _():
                row_copy(0, block, part, z).wait_send()

            @pl.when((z <= block) & (z > 0))
            def _():
                row_copy(1, block, part, z).wait_send()

    for part in range(chain):
        for block in range(line):

            @pl.when(z != block)
            def _():
                chain_copy(0, block, part, z).wait_send()

    for j in range(line):
        for i in range(1, plane):
            select_copy(j, i).wait_send()
        partner_copy(j).wait_send()
        for h in range(halves):
            partial_copy(j, h).wait_send()
            for i in range(1, plane):
                return_copy(j, i, h).wait_send()


def run_layer(inputs, small, weights, cap):
    queries, keys, values, gates, project, residual = inputs
    decay, gain, norm, route, cos, sin = small
    count = lax.axis_size("sp")
    line = line_length(count)
    plane = count // line
    length, channels = queries.shape
    tokens, width = residual.shape
    heads, lanes = decay.shape[1], cos.shape[1]
    size = channels // heads
    groups = channels // lanes
    slice_rows = groups * size // plane
    inner = weights[0].shape[2]
    slots = plane * cap
    parts, halves, chain = 2, 2, 4
    bf16, f32 = jnp.bfloat16, jnp.float32
    dma = pltpu.SemaphoreType.DMA
    vmem = pl.BlockSpec(memory_space=pltpu.VMEM)
    hbm = pl.BlockSpec(memory_space=pl.ANY)
    return pl.pallas_call(
        functools.partial(layer_kernel, line, plane, cap, parts, halves, chain),
        out_shape=jax.ShapeDtypeStruct((tokens, width), bf16),
        in_specs=[hbm] * 4 + [vmem] * 2 + [hbm] * 2 + [vmem] * 4 + [hbm] * 3,
        out_specs=vmem,
        scratch_shapes=[
            pltpu.VMEM((length, channels), bf16),
            pltpu.VMEM((length, channels), bf16),
            pltpu.VMEM((length, channels), bf16),
            pltpu.VMEM((length, channels), bf16),
            pltpu.VMEM((channels, width), bf16),
            pltpu.VMEM((tokens, width), bf16),
            pltpu.VMEM((length, channels), f32),
            pltpu.VMEM((heads, length), f32),
            pltpu.VMEM((length, channels), bf16),
            pltpu.VMEM((length, channels), bf16),
            pltpu.VMEM((length, channels), bf16),
            pltpu.VMEM((length, channels), f32),
            pltpu.VMEM((length, channels), bf16),
            pltpu.VMEM((tokens, width), bf16),
            pltpu.VMEM((tokens, width), bf16),
            pltpu.VMEM((tokens, width), bf16),
            pltpu.VMEM(route.shape, f32),
            pltpu.VMEM((plane, slice_rows, lanes), bf16),
            pltpu.VMEM((plane, slice_rows, lanes), bf16),
            pltpu.VMEM((plane, groups, 8, lanes), f32),
            pltpu.VMEM((plane, slice_rows, lanes), f32),
            pltpu.VMEM((slice_rows, lanes), bf16),
            pltpu.VMEM((8, lanes), f32),
            pltpu.VMEM((line, slice_rows, lanes), bf16),
            pltpu.VMEM((line, 8, lanes), f32),
            pltpu.VMEM((slice_rows, lanes), f32),
            pltpu.VMEM((plane, slice_rows, lanes), bf16),
            pltpu.VMEM((plane, slice_rows, lanes), bf16),
            dma((6,)),
            dma((plane,)),
            dma((plane,)),
            dma((plane,)),
            dma((plane,)),
            dma((line, 2)),
            dma((line, 2)),
            dma((plane,)),
            dma((plane,)),
            dma((2,)),
            dma((2,)),
            pltpu.VMEM((width, inner), bf16),
            pltpu.VMEM((width, inner), bf16),
            pltpu.VMEM((inner, width), bf16),
            pltpu.VMEM((line, tokens, width), bf16),
            pltpu.VMEM((line,) + route.shape, f32),
            pltpu.VMEM((line, plane, cap, width), bf16),
            pltpu.VMEM((line, 2, plane, cap, width), bf16),
            pltpu.VMEM((2 * slots, inner), bf16),
            pltpu.VMEM((line, 2, plane, cap, width), bf16),
            pltpu.VMEM((line, plane, cap, width), bf16),
            pltpu.VMEM((line, plane, cap, width), bf16),
            pltpu.VMEM((line, plane, cap, width), bf16),
            pltpu.VMEM((line, tokens, width), f32),
            pltpu.VMEM((line, tokens, width), bf16),
            pltpu.VMEM((2, line, tokens, width), bf16),
            dma((3, 4)),
            dma((2, line, parts)),
            dma((line, parts)),
            dma((line,)),
            dma((line,)),
            dma((line, plane)),
            dma((line, plane)),
            dma((line,)),
            dma((line,)),
            dma((line, halves)),
            dma((line, halves)),
            dma((line, plane, halves)),
            dma((line, plane, halves)),
            dma((line, chain)),
            dma((2, line, chain)),
        ],
        compiler_params=pltpu.CompilerParams(
            collective_id=1, has_side_effects=True, vmem_limit_bytes=67043328
        ),
        name="layer",
    )(
        queries,
        keys,
        values,
        gates,
        decay,
        gain,
        project,
        residual,
        norm,
        route,
        cos,
        sin,
        *weights,
    )


def shards(
    queries,
    key_vectors,
    value_vectors,
    gate_inputs,
    log_decay,
    head_gain,
    out_weight,
    residual,
    norm_gain,
    expert_ids,
    expert_weights,
    gate_experts,
    up_experts,
    down_experts,
):
    tok_dev, channels = queries.shape
    head_size = channels // log_decay.shape[1]
    lanes = 128
    places = lax.axis_index("sp") * tok_dev + jnp.arange(tok_dev, dtype=jnp.int32)
    half_size = head_size // 2
    frequency = 10000.0 ** (-jnp.arange(half_size, dtype=jnp.float32) / half_size)
    angles = places.astype(jnp.float32)[:, None] * jnp.tile(frequency, lanes // half_size)
    sign = jnp.where(jnp.arange(lanes) % head_size < half_size, -1.0, 1.0)
    top_count = expert_ids.shape[1]
    route = jnp.concatenate(
        [
            expert_ids.T.astype(jnp.float32),
            expert_weights.T,
            jnp.zeros((8 - 2 * top_count, expert_ids.shape[0]), jnp.float32),
        ],
        axis=0,
    )
    return run_layer(
        (queries, key_vectors, value_vectors, gate_inputs, out_weight, residual),
        (
            log_decay,
            head_gain[None, :],
            norm_gain[None, :],
            route,
            jnp.cos(angles),
            jnp.sin(angles) * sign,
        ),
        (gate_experts, up_experts, down_experts),
        2 * tok_dev // lax.axis_size("sp"),
    )


def solution(mesh):
    return jax.shard_map(
        shards,
        mesh=mesh,
        in_specs=(
            P("sp", "tp"),
            P("sp", "tp"),
            P("sp", "tp"),
            P("sp", "tp"),
            P("sp", "tp"),
            P("tp"),
            P("tp", None),
            P(("sp", "tp"), None),
            P(),
            P(("sp", "tp"), None),
            P(("sp", "tp"), None),
            P("sp", None, "tp"),
            P("sp", None, "tp"),
            P("sp", "tp", None),
        ),
        out_specs=P(("sp", "tp"), None),
        check_vma=False,
    )
```

```python
import functools

import jax
import jax.numpy as jnp
from jax import lax
from jax.experimental import pallas as pl
from jax.experimental.pallas import tpu as pltpu
from jax.sharding import PartitionSpec as P

MESH = pl.DeviceIdType.MESH


def line_length(count):
    size = 1
    while size * size * size < count:
        size *= 2
    return size


def layer_kernel(
    line,
    plane,
    cap,
    parts,
    halves,
    chain,
    query_hbm,
    key_hbm,
    value_hbm,
    gates_hbm,
    decay_ref,
    gain_ref,
    project_hbm,
    residual_hbm,
    norm_ref,
    ids_ref,
    shares_ref,
    gate_hbm,
    up_hbm,
    down_hbm,
    out_ref,
    query_ref,
    key_ref,
    value_ref,
    gates_ref,
    project_ref,
    residual_ref,
    cos_ref,
    sin_ref,
    running_ref,
    by_head_ref,
    turned_query,
    turned_key,
    start_query,
    within_ref,
    normed_ref,
    away_ref,
    got_ref,
    mixed_ref,
    meta_ref,
    state_out,
    state_in,
    totals,
    before_ref,
    plane_state,
    plane_total,
    line_state,
    line_total,
    carry_ref,
    back_state,
    start_state,
    lsem,
    asend,
    arecv,
    bsend,
    brecv,
    ctsend,
    ctrecv,
    dsend,
    drecv,
    esend,
    erecv,
    gate_ref,
    up_ref,
    down_ref,
    zbuf,
    meta,
    sel,
    xbuf,
    hidden,
    ybuf,
    yin,
    sbuf,
    rbuf,
    cbuf,
    csend,
    pin,
    wsem,
    zsend,
    zrecv,
    msend,
    mrecv,
    psend,
    precv,
    tsend,
    trecv,
    ysend,
    yrecv,
    rsend,
    rrecv,
    ssend,
    srecv,
):
    sp, core = lax.axis_index("sp"), lax.axis_index("tp")
    z, p = sp // plane, lax.rem(sp, plane)
    length, channels = query_ref.shape
    tokens, width = residual_ref.shape
    lanes = cos_ref.shape[1]
    heads = decay_ref.shape[0]
    size = channels // heads
    pack = lanes // size
    groups = channels // lanes
    slice_rows = state_out.shape[1]
    slots = plane * cap
    f32, bf16 = jnp.float32, jnp.bfloat16

    def at(line_place, plane_place):
        return {"sp": line_place * plane + plane_place, "tp": core}

    partner = {"sp": sp, "tp": 1 - core}

    def remote(src, dst, send, recv, device):
        return pltpu.make_async_remote_copy(
            src_ref=src,
            dst_ref=dst,
            send_sem=send,
            recv_sem=recv,
            device_id=device,
            device_id_type=MESH,
        )

    loads = [
        pltpu.make_async_copy(source, target, lsem.at[number])
        for number, (source, target) in enumerate(
            (
                (query_hbm, query_ref),
                (key_hbm, key_ref),
                (value_hbm, value_ref),
                (gates_hbm, gates_ref),
                (project_hbm, project_ref),
                (residual_hbm, residual_ref),
            )
        )
    ]
    for copy in loads:
        copy.start()

    weights = []
    for number, (source, target) in enumerate(
        ((gate_hbm, gate_ref), (up_hbm, up_ref), (down_hbm, down_ref))
    ):
        depth = target.shape[0] // 4
        for piece in range(4):
            part = pl.ds(piece * depth, depth)
            weights.append(
                pltpu.make_async_copy(
                    source.at[0, part], target.at[part], wsem.at[number, piece]
                )
            )

    barrier = pltpu.get_barrier_semaphore()
    peers = [at(lax.rem(z + i, line), p) for i in range(1, line)]
    peers += [at(z, lax.rem(p + i, plane)) for i in range(1, plane)] + [partner]
    for peer in peers:
        pl.semaphore_signal(barrier, inc=1, device_id=peer, device_id_type=MESH)
    for copy in weights:
        copy.start()

    lane = lax.broadcasted_iota(jnp.int32, (1, lanes), 1)
    contract = (((1,), (1,)), ((), ()))
    upright = (((0,), (0,)), ((), ()))

    def place_of(group):
        return pl.ds(pl.multiple_of(group * lanes, lanes), lanes)

    def by_lane(pieces):
        value = pieces[-1]
        for number in range(pack - 2, -1, -1):
            value = jnp.where(lane < (number + 1) * size, pieces[number], value)
        return value

    count = line * plane
    with jax.named_scope("slots"):
        expert = lax.broadcasted_iota(jnp.int32, (count, tokens), 0).astype(f32)
        first, second = ids_ref[0:1, :].astype(f32), ids_ref[1:2, :].astype(f32)
        first_hot = jnp.where(expert == first, 1.0, 0.0)
        second_hot = jnp.where(expert == second, 1.0, 0.0)
        earlier = lax.broadcasted_iota(jnp.int32, (tokens, tokens), 0) < (
            lax.broadcasted_iota(jnp.int32, (tokens, tokens), 1)
        )
        taken = jnp.dot(
            (first_hot + second_hot).astype(bf16),
            jnp.where(earlier, 1.0, 0.0).astype(bf16),
            preferred_element_type=f32,
        )
        first_rank = jnp.sum(first_hot * taken, axis=0, keepdims=True)
        second_rank = jnp.sum(second_hot * taken, axis=0, keepdims=True)
        meta_ref[...] = jnp.zeros_like(meta_ref)
        meta_ref[0:1, :] = first * cap + first_rank
        meta_ref[1:2, :] = second * cap + second_rank
        meta_ref[2:4, :] = shares_ref[...]

    with jax.named_scope("running"):
        rows_of = lax.broadcasted_iota(jnp.int32, (length, length), 0)
        columns_of = lax.broadcasted_iota(jnp.int32, (length, length), 1)
        causal = rows_of >= columns_of
        lower = jnp.where(causal, 1.0, 0.0).astype(bf16)
        upper = jnp.where(rows_of <= columns_of, 1.0, 0.0).astype(bf16)
        spread = lax.broadcasted_iota(jnp.int32, (heads, channels), 1) // size == (
            lax.broadcasted_iota(jnp.int32, (heads, channels), 0)
        )
        spread = jnp.where(spread, 1.0, 0.0).astype(bf16)
        rest = decay_ref[...]
        running, by_head = 0.0, 0.0
        for _ in range(3):
            piece = rest.astype(bf16)
            rest = rest - piece.astype(f32)
            wide_piece = lax.dot_general(piece, spread, upright, preferred_element_type=f32)
            wide_piece = wide_piece.astype(bf16)
            running = running + jnp.dot(lower, wide_piece, preferred_element_type=f32)
            by_head = by_head + jnp.dot(piece, upper, preferred_element_type=f32)
        running_ref[...] = running
        by_head_ref[...] = by_head

    swapped = lax.broadcasted_iota(jnp.int32, (lanes, lanes), 0) == (
        lax.broadcasted_iota(jnp.int32, (lanes, lanes), 1) ^ (size // 2)
    )
    swapped = jnp.where(swapped, 1.0, 0.0).astype(bf16)
    with jax.named_scope("table"):
        half_size = size // 2
        step_of = lane % half_size
        frequency = jnp.zeros((1, lanes), f32)
        for number in range(half_size):
            constant = float(10000.0 ** (-number / half_size))
            frequency = jnp.where(step_of == number, constant, frequency)
        fine = 16
        row = lax.broadcasted_iota(jnp.int32, (fine, lanes), 0)
        near_angle = row.astype(f32) * frequency
        near_cos, near_sin = jnp.cos(near_angle), jnp.sin(near_angle)
        rounds = length // fine
        row = lax.broadcasted_iota(jnp.int32, (rounds, lanes), 0)
        far_angle = (sp * length + row * fine).astype(f32) * frequency
        far_cos, far_sin = jnp.cos(far_angle), jnp.sin(far_angle)
        sign = jnp.where(lane % size < half_size, -1.0, 1.0)
        for number in range(rounds):
            some = pl.ds(number * fine, fine)
            a, b = far_cos[number : number + 1, :], far_sin[number : number + 1, :]
            cos_ref[some, :] = a * near_cos - b * near_sin
            sin_ref[some, :] = (b * near_cos + a * near_sin) * sign

    with jax.named_scope("loadw"):
        for copy in loads[:3]:
            copy.wait()

    def turn(block):
        other = jnp.dot(block, swapped, preferred_element_type=f32)
        return block.astype(f32) * cos_ref[...] + other * sin_ref[...]

    with jax.named_scope("turn"):
        for group in range(groups):
            where = pl.ds(group * lanes, lanes)
            run = running_ref[:, where]
            query = turn(query_ref[:, where])
            key = turn(key_ref[:, where]) * size ** (-0.5)
            turned_query[:, where] = query.astype(bf16)
            turned_key[:, where] = key.astype(bf16)
            start_query[:, where] = (query * jnp.exp(run)).astype(bf16)
            end = run[length - 1 : length, :]
            final = lax.dot_general(
                (key * jnp.exp(end - run)).astype(bf16),
                value_ref[:, where],
                upright,
                preferred_element_type=f32,
            )
            state = by_lane([final[n * size : (n + 1) * size, :] for n in range(pack)])
            totals[p, group] = jnp.broadcast_to(end, totals.shape[2:])
            per = size // slice_rows if slice_rows < size else 1
            deep = min(slice_rows, size)
            for part in range(per):
                row = group * size + part * deep
                state_out[row // slice_rows, pl.ds(row % slice_rows, deep), :] = state[
                    part * deep : (part + 1) * deep, :
                ].astype(bf16)
        state_in[p] = state_out[p]

    with jax.named_scope("barrier"):
        pl.semaphore_wait(barrier, len(peers))

    def state_copy(i):
        q = lax.rem(p + i, plane)
        return remote(
            state_out.at[q], state_in.at[p], asend.at[i], arecv.at[i], at(z, q)
        )

    def total_copy(i):
        q = lax.rem(p + i, plane)
        return remote(totals.at[p], totals.at[p], bsend.at[i], brecv.at[i], at(z, q))

    for i in range(1, plane):
        state_copy(i).start()
        total_copy(i).start()

    def meta_copy(i):
        return remote(
            meta_ref, meta.at[z], msend.at[i], mrecv.at[i], at(lax.rem(z + i, line), p)
        )

    for i in range(1, line):
        meta_copy(i).start()

    def attend(lo, hi):
        @pl.loop(lo, hi)
        def _(group):
            where = place_of(group)
            query, key, value = turned_query[:, where], turned_key[:, where], value_ref[:, where]
            run = running_ref[:, where]
            total = []
            for number in range(pack):
                mine = (lane >= number * size) & (lane < (number + 1) * size)
                masked = jnp.where(mine, query, jnp.zeros_like(query))
                score = lax.dot_general(masked, key, contract, preferred_element_type=f32)
                gap = run[:, number * size : number * size + 1] - by_head_ref[
                    pl.ds(group * pack + number, 1), :
                ]
                ok = lax.broadcasted_iota(jnp.int32, (length, length), 0) >= (
                    lax.broadcasted_iota(jnp.int32, (length, length), 1)
                )
                weight = jnp.where(ok, jnp.exp(jnp.where(ok, gap, 0.0)), 0.0)
                total.append(
                    jnp.dot((score * weight).astype(bf16), value, preferred_element_type=f32)
                )
            within_ref[:, where] = by_lane(total)

    with jax.named_scope("attendA"):
        attend(0, groups // 2)

    mine = p * slice_rows // size
    with jax.named_scope("wait1"):
        for i in range(1, plane):
            state_copy(i).wait_recv()
            total_copy(i).wait_recv()

    held = jnp.zeros((slice_rows, lanes), f32)
    elapsed = jnp.zeros((1, lanes), f32)
    for q in range(plane):
        before_ref[q] = held
        step = totals[q, mine][0:1, :]
        held = jnp.exp(step) * held + state_in[q].astype(f32)
        elapsed = elapsed + step
    plane_state[...] = held.astype(bf16)
    plane_total[...] = jnp.broadcast_to(elapsed, plane_total.shape)

    def line_state_copy(i):
        return remote(
            plane_state, line_state.at[z], ctsend.at[i, 0], ctrecv.at[i, 0], at(z + i, p)
        )

    def line_total_copy(i):
        return remote(
            plane_total, line_total.at[z], ctsend.at[i, 1], ctrecv.at[i, 1], at(z + i, p)
        )

    for i in range(1, line):

        @pl.when(z + i < line)
        def _():
            line_state_copy(i).start()
            line_total_copy(i).start()

    with jax.named_scope("attendB"):
        attend(groups // 2, groups)

    with jax.named_scope("wait2"):
        carry_ref[...] = jnp.zeros_like(carry_ref)
        for i in range(line - 1, 0, -1):

            @pl.when(z >= i)
            def _():
                line_state_copy(i).wait_recv()
                line_total_copy(i).wait_recv()
                step = line_total[z - i][0:1, :]
                carry_ref[...] = jnp.exp(step) * carry_ref[...] + line_state[z - i].astype(f32)

    elapsed = jnp.zeros((1, lanes), f32)
    for q in range(plane):
        value = before_ref[q] + jnp.exp(elapsed) * carry_ref[...]
        back_state[q] = value.astype(bf16)
        elapsed = elapsed + totals[q, mine][0:1, :]

    def start_copy(i):
        q = lax.rem(p + i, plane)
        return remote(
            back_state.at[q], start_state.at[p], dsend.at[i], drecv.at[i], at(z, q)
        )

    for i in range(1, plane):
        start_copy(i).start()
    start_state[p] = back_state[p]
    with jax.named_scope("wait3"):
        for copy in loads[3:]:
            copy.wait()
        for i in range(1, plane):
            start_copy(i).wait_recv()

    with jax.named_scope("epilogue"):
        for group in range(groups):
            where = pl.ds(group * lanes, lanes)
            pieces = []
            for part in range(max(1, size // slice_rows)):
                row = group * size + part * slice_rows
                deep = min(slice_rows, size)
                pieces.append(start_state[row // slice_rows, pl.ds(row % slice_rows, deep), :])
            state = pieces[0] if len(pieces) == 1 else jnp.concatenate(pieces, axis=0)
            diagonal = jnp.concatenate(
                [
                    jnp.where(
                        (lane >= n * size) & (lane < (n + 1) * size), state, jnp.zeros_like(state)
                    )
                    for n in range(pack)
                ],
                axis=0,
            )
            retained = within_ref[:, where] + jnp.dot(
                start_query[:, where], diagonal, preferred_element_type=f32
            )
            square = retained * retained
            sums = [
                jnp.sum(
                    jnp.where((lane >= n * size) & (lane < (n + 1) * size), square, 0.0),
                    axis=1,
                    keepdims=True,
                )
                for n in range(pack)
            ]
            mean = by_lane(sums) * (1.0 / size)
            gates = gates_ref[:, where].astype(f32)
            normed = retained * lax.rsqrt(mean + 1e-06) * gain_ref[:, where]
            normed = normed * (gates / (1.0 + jnp.exp(-gates)))
            normed_ref[:, where] = normed.astype(bf16)

    def away_copy(h):
        columns = pl.ds(h * (width // 2), width // 2)
        return remote(
            away_ref.at[:, columns], got_ref.at[:, columns], esend.at[h], erecv.at[h], partner
        )

    away_rows = pl.ds(pl.multiple_of((1 - core) * tokens, tokens), tokens)
    here_rows = pl.ds(pl.multiple_of(core * tokens, tokens), tokens)
    with jax.named_scope("proj"):
        for h in range(2):
            columns = pl.ds(h * (width // 2), width // 2)
            away_ref[:, columns] = jnp.dot(
                normed_ref[away_rows, :], project_ref[:, columns], preferred_element_type=f32
            ).astype(bf16)
            away_copy(h).start()
        squares = jnp.zeros((tokens, 1), f32)
        for h in range(2):
            columns = pl.ds(h * (width // 2), width // 2)
            here = jnp.dot(
                normed_ref[here_rows, :], project_ref[:, columns], preferred_element_type=f32
            ).astype(bf16)
            away_copy(h).wait_recv()
            projected = here.astype(f32) + got_ref[:, columns].astype(f32)
            mixed = (residual_ref[:, columns].astype(f32) + projected).astype(bf16)
            mixed_ref[:, columns] = mixed
            mixed = mixed.astype(f32)
            squares = squares + jnp.sum(mixed * mixed, axis=1, keepdims=True)
        scale = lax.rsqrt(squares * (1.0 / width) + 1e-06)
        for h in range(2):
            columns = pl.ds(h * (width // 2), width // 2)
            normed = mixed_ref[:, columns].astype(f32) * scale * norm_ref[:, columns]
            zbuf[z, :, columns] = normed.astype(bf16)

    piece_rows = tokens // parts
    chain_width = width // chain

    def row_copy(way, block, part, target):
        rows = pl.ds(part * piece_rows, piece_rows)
        return remote(
            zbuf.at[block, rows],
            zbuf.at[block, rows],
            zsend.at[way, block, part],
            zrecv.at[block, part],
            at(target, p),
        )

    for part in range(parts):

        @pl.when(z + 1 < line)
        def _():
            row_copy(0, z, part, z + 1).start()

        @pl.when(z > 0)
        def _():
            row_copy(1, z, part, z - 1).start()

    meta[z] = meta_ref[...]

    near = jnp.minimum(z, line - 1 - z)
    longer_up = z < line - 1 - z

    def block_of(place):
        both = place <= 2 * near
        away = jnp.where(both, (place + 1) // 2, place - near)
        forward = jnp.where(both, place % 2 == 1, longer_up)
        return jnp.where(forward, z + away, z - away)

    def pass_on(distance, lo, hi):
        for part in range(lo, hi):
            low, high = z - distance, z + distance

            @pl.when(low >= 0)
            def _():
                row_copy(0, low, part, z).wait_recv()

                @pl.when(z + 1 < line)
                def _():
                    row_copy(0, low, part, z + 1).start()

            @pl.when(high < line)
            def _():
                row_copy(1, high, part, z).wait_recv()

                @pl.when(z > 0)
                def _():
                    row_copy(1, high, part, z - 1).start()

    def slot_names():
        names = lax.broadcasted_iota(jnp.int32, (slots, tokens), 0) + z * slots
        return names.astype(f32)

    def select_copy(j, i):
        q = lax.rem(p + i, plane)
        return remote(
            sel.at[j, q], xbuf.at[j, core, p], psend.at[j, i], precv.at[j, i], at(z, q)
        )

    def partner_copy(j, i):
        q = lax.rem(p + plane - i, plane)
        return remote(
            xbuf.at[j, core, q], xbuf.at[j, core, q], tsend.at[j, i], trecv.at[j, i], partner
        )

    def select(j):
        block = block_of(j)
        names = slot_names()
        chosen = (names == meta[block, 0:1, :]) | (names == meta[block, 1:2, :])
        place = jnp.where(chosen, 1.0, 0.0).astype(bf16)
        picked = jnp.dot(place, zbuf[block], preferred_element_type=f32)
        sel[j] = picked.reshape(plane, cap, width).astype(bf16)
        for i in range(1, plane):
            select_copy(j, i).start()
        xbuf[j, core, p] = sel[j, p]
        partner_copy(j, 0).start()

    def collect(j):
        for i in range(1, plane):
            select_copy(j, i).wait_recv()
            partner_copy(j, i).start()

    half = width // halves

    def partial_copy(j, h):
        columns = pl.ds(h * half, half)
        return remote(
            ybuf.at[j, 1 - core, :, :, columns],
            yin.at[j, :, :, columns],
            ysend.at[j, h],
            yrecv.at[j, h],
            partner,
        )

    tall = 2 * slots
    wide = 256

    def widen(j, lo, hi):
        if lo == hi:
            return
        if cap % 16 == 0:
            batch = xbuf[j].reshape(tall, width)
        else:
            batch = xbuf[j].astype(f32).reshape(tall, width).astype(bf16)

        for tile in range(lo, hi):
            columns = pl.ds(tile * wide, wide)
            gate = jnp.dot(batch, gate_ref[:, columns], preferred_element_type=f32)
            up = jnp.dot(batch, up_ref[:, columns], preferred_element_type=f32)
            hidden[:, columns] = (gate * up / (1.0 + jnp.exp(-gate))).astype(bf16)

    def narrow(j, h):
        for tile in range(h * (half // wide), (h + 1) * (half // wide)):
            columns = pl.ds(tile * wide, wide)
            value = jnp.dot(hidden[...], down_ref[:, columns], preferred_element_type=f32)
            ybuf[j, :, :, :, columns] = value.reshape(2, plane, cap, wide).astype(bf16)

        partial_copy(j, h).start()

    def return_copy(j, i, h):
        q = lax.rem(p + i, plane)
        columns = pl.ds(h * half, half)
        return remote(
            sbuf.at[j, q, :, columns],
            rbuf.at[j, p, :, columns],
            rsend.at[j, i, h],
            rrecv.at[j, i, h],
            at(z, q),
        )

    def give_back(j, h):
        columns = pl.ds(h * half, half)
        partial_copy(j, h).wait_recv()
        total = ybuf[j, core, :, :, columns].astype(f32) + yin[j, :, :, columns].astype(f32)
        sbuf[j, :, :, columns] = total.astype(bf16)
        for i in range(1, plane):
            return_copy(j, i, h).start()
        rbuf[j, p, :, columns] = sbuf[j, p, :, columns]

    def chain_copy(way, block, part, target):
        columns = pl.ds(part * chain_width, chain_width)
        return remote(
            csend.at[block, :, columns],
            pin.at[way, block, :, columns],
            ssend.at[block, part],
            srecv.at[way, block, part],
            at(target, p),
        )

    def weigh_of(j):
        block = block_of(j)
        names = slot_names()
        weigh = jnp.where(names == meta[block, 0:1, :], meta[block, 2:3, :], 0.0)
        weigh = weigh + jnp.where(names == meta[block, 1:2, :], meta[block, 3:4, :], 0.0)
        weigh = weigh.T
        high = weigh.astype(bf16)
        return high, (weigh - high.astype(f32)).astype(bf16)

    def combine(j, h, weigh):
        for i in range(1, plane):
            return_copy(j, i, h).wait_recv()
        block = block_of(j)
        high, low = weigh
        columns = pl.ds(h * half, half)
        if cap % 16 == 0:
            back = rbuf[j, :, :, columns].reshape(slots, half)
        else:
            back = rbuf[j, :, :, columns].astype(f32).reshape(slots, half).astype(bf16)
        total = jnp.dot(high, back, preferred_element_type=f32) + jnp.dot(
            low, back, preferred_element_type=f32
        )
        if j == 0:
            cbuf[block, :, columns] = total + mixed_ref[:, columns].astype(f32)
        else:
            cbuf[block, :, columns] = total

            @pl.when((z == 0) | (z == line - 1))
            def _():
                csend[block, :, columns] = total.astype(bf16)

            for part in range(h * chain // halves, (h + 1) * chain // halves):

                @pl.when(z == 0)
                def _():
                    chain_copy(0, block, part, z + 1).start()

                @pl.when(z == line - 1)
                def _():
                    chain_copy(1, block, part, z - 1).start()

    def relay(way, block, part):
        before = jnp.where(way == 0, z < block, z > block)
        inside = before & (z > 0) & (z < line - 1)
        columns = pl.ds(part * chain_width, chain_width)

        @pl.when(inside)
        def _():
            chain_copy(way, block, part, z).wait_recv()
            total = cbuf[block, :, columns] + pin[way, block, :, columns].astype(f32)
            csend[block, :, columns] = total.astype(bf16)
            chain_copy(way, block, part, z + 1 - 2 * way).start()

    first_way = jnp.where(2 * z < line, 0, 1)

    def relays(i, lo, hi):
        def one(way, part):
            relay(way, jnp.where(way == 0, i, line - 1 - i), part)

        for part in range(lo, hi + lag):
            if part < hi:
                one(first_way, part)
            if part >= lo + lag:
                one(1 - first_way, part - lag)

    lag = chain // 2
    tiles = hidden.shape[1] // wide
    sc = jax.named_scope
    with sc("select#0"):
        select(0)
    with sc("meta"):
        for i in range(1, line):
            meta_copy(i).wait_recv()
    with sc("pass#1a"):
        pass_on(1, 0, parts // 2)
    with sc("collect#0"):
        collect(0)
    for j in range(line):
        last = j + 1 == line
        cut = tiles if last else (tiles + j) // 2
        with sc(f"xwait#{j}"):
            for i in range(plane):
                partner_copy(j, i).wait_recv()
            if j == 0:
                for copy in weights:
                    copy.wait()
        with sc(f"widen#{j}a"):
            widen(j, 0, cut)
        if not last:
            with sc(f"pass#{j + 1}b"):
                pass_on(j + 1, parts // 2, parts)
            with sc(f"select#{j + 1}"):
                select(j + 1)
        with sc(f"widen#{j}b"):
            widen(j, cut, tiles)
        if j >= 2 and last:
            with sc(f"combine#{j - 1}"):
                weigh = weigh_of(j - 1)
                for h in range(halves):
                    combine(j - 1, h, weigh)
        with sc(f"narrow#{j}a"):
            narrow(j, 0)
        if j >= 2 and not last:
            with sc(f"combine#{j - 1}"):
                weigh = weigh_of(j - 1)
                for h in range(halves):
                    combine(j - 1, h, weigh)
        with sc(f"narrow#{j}b"):
            for h in range(1, halves):
                narrow(j, h)
        if j + 2 < line:
            with sc(f"pass#{j + 2}a"):
                pass_on(j + 2, 0, parts // 2)
        if j >= 1:
            with sc(f"give#{j}"):
                for h in range(halves):
                    give_back(j, h)
        if j == max(0, line - 2):
            with sc("give#0"):
                for h in range(halves):
                    give_back(0, h)
        if not last:
            with sc(f"collect#{j + 1}"):
                collect(j + 1)
        if 2 <= j < line - 2:
            relays(j, 0, chain)
    weigh = weigh_of(line - 1)
    share = chain // halves
    for h in range(halves):
        if line > 2:
            with sc(f"relays#a{h}"):
                relays(line - 2, h * share, h * share + share // 2)
        with sc(f"combine#last{h}"):
            combine(line - 1, h, weigh)
        if line > 2:
            with sc(f"relays#b{h}"):
                relays(line - 2, h * share + share // 2, (h + 1) * share)
    with sc("relays#c"):
        relays(line - 1, 0, chain)
    with sc("combine#own"):
        weigh = weigh_of(0)
        for h in range(halves):
            combine(0, h, weigh)
    with sc("own"):
        for part in range(chain):
            columns = pl.ds(part * chain_width, chain_width)

            @pl.when(z > 0)
            def _():
                chain_copy(0, z, part, z).wait_recv()
                cbuf[z, :, columns] = cbuf[z, :, columns] + pin[0, z, :, columns].astype(f32)

            @pl.when(z < line - 1)
            def _():
                chain_copy(1, z, part, z).wait_recv()
                cbuf[z, :, columns] = cbuf[z, :, columns] + pin[1, z, :, columns].astype(f32)

    out_ref[...] = cbuf[z].astype(bf16)

    for i in range(1, line):
        meta_copy(i).wait_send()

        @pl.when(z + i < line)
        def _():
            line_state_copy(i).wait_send()
            line_total_copy(i).wait_send()

    for i in range(1, plane):
        state_copy(i).wait_send()
        total_copy(i).wait_send()
        start_copy(i).wait_send()
    for h in range(2):
        away_copy(h).wait_send()
    for part in range(parts):
        for block in range(line):

            @pl.when((z >= block) & (z + 1 < line))
            def _():
                row_copy(0, block, part, z).wait_send()

            @pl.when((z <= block) & (z > 0))
            def _():
                row_copy(1, block, part, z).wait_send()

    for part in range(chain):
        for block in range(line):

            @pl.when(z != block)
            def _():
                chain_copy(0, block, part, z).wait_send()

    for j in range(line):
        for i in range(1, plane):
            select_copy(j, i).wait_send()
        for i in range(plane):
            partner_copy(j, i).wait_send()
        for h in range(halves):
            partial_copy(j, h).wait_send()
            for i in range(1, plane):
                return_copy(j, i, h).wait_send()


def run_layer(inputs, small, weights, cap):
    queries, keys, values, gates, project, residual = inputs
    decay, gain, norm, ids, shares = small
    lanes = 128
    count = lax.axis_size("sp")
    line = line_length(count)
    plane = count // line
    length, channels = queries.shape
    tokens, width = residual.shape
    heads = decay.shape[0]
    size = channels // heads
    groups = channels // lanes
    slice_rows = groups * size // plane
    inner = weights[0].shape[2]
    slots = plane * cap
    parts, halves, chain = 2, 2, 4
    bf16, f32 = jnp.bfloat16, jnp.float32
    dma = pltpu.SemaphoreType.DMA
    vmem = pl.BlockSpec(memory_space=pltpu.VMEM)
    hbm = pl.BlockSpec(memory_space=pl.ANY)
    return pl.pallas_call(
        functools.partial(layer_kernel, line, plane, cap, parts, halves, chain),
        out_shape=jax.ShapeDtypeStruct((tokens, width), bf16),
        in_specs=[hbm] * 4 + [vmem] * 2 + [hbm] * 2 + [vmem] * 3 + [hbm] * 3,
        out_specs=vmem,
        scratch_shapes=[
            pltpu.VMEM((length, channels), bf16),
            pltpu.VMEM((length, channels), bf16),
            pltpu.VMEM((length, channels), bf16),
            pltpu.VMEM((length, channels), bf16),
            pltpu.VMEM((channels, width), bf16),
            pltpu.VMEM((tokens, width), bf16),
            pltpu.VMEM((length, lanes), f32),
            pltpu.VMEM((length, lanes), f32),
            pltpu.VMEM((length, channels), f32),
            pltpu.VMEM((heads, length), f32),
            pltpu.VMEM((length, channels), bf16),
            pltpu.VMEM((length, channels), bf16),
            pltpu.VMEM((length, channels), bf16),
            pltpu.VMEM((length, channels), f32),
            pltpu.VMEM((length, channels), bf16),
            pltpu.VMEM((tokens, width), bf16),
            pltpu.VMEM((tokens, width), bf16),
            pltpu.VMEM((tokens, width), bf16),
            pltpu.VMEM((8, tokens), f32),
            pltpu.VMEM((plane, slice_rows, lanes), bf16),
            pltpu.VMEM((plane, slice_rows, lanes), bf16),
            pltpu.VMEM((plane, groups, 8, lanes), f32),
            pltpu.VMEM((plane, slice_rows, lanes), f32),
            pltpu.VMEM((slice_rows, lanes), bf16),
            pltpu.VMEM((8, lanes), f32),
            pltpu.VMEM((line, slice_rows, lanes), bf16),
            pltpu.VMEM((line, 8, lanes), f32),
            pltpu.VMEM((slice_rows, lanes), f32),
            pltpu.VMEM((plane, slice_rows, lanes), bf16),
            pltpu.VMEM((plane, slice_rows, lanes), bf16),
            dma((6,)),
            dma((plane,)),
            dma((plane,)),
            dma((plane,)),
            dma((plane,)),
            dma((line, 2)),
            dma((line, 2)),
            dma((plane,)),
            dma((plane,)),
            dma((2,)),
            dma((2,)),
            pltpu.VMEM((width, inner), bf16),
            pltpu.VMEM((width, inner), bf16),
            pltpu.VMEM((inner, width), bf16),
            pltpu.VMEM((line, tokens, width), bf16),
            pltpu.VMEM((line, 8, tokens), f32),
            pltpu.VMEM((line, plane, cap, width), bf16),
            pltpu.VMEM((line, 2, plane, cap, width), bf16),
            pltpu.VMEM((2 * slots, inner), bf16),
            pltpu.VMEM((line, 2, plane, cap, width), bf16),
            pltpu.VMEM((line, plane, cap, width), bf16),
            pltpu.VMEM((line, plane, cap, width), bf16),
            pltpu.VMEM((line, plane, cap, width), bf16),
            pltpu.VMEM((line, tokens, width), f32),
            pltpu.VMEM((line, tokens, width), bf16),
            pltpu.VMEM((2, line, tokens, width), bf16),
            dma((3, 4)),
            dma((2, line, parts)),
            dma((line, parts)),
            dma((line,)),
            dma((line,)),
            dma((line, plane)),
            dma((line, plane)),
            dma((line, plane)),
            dma((line, plane)),
            dma((line, halves)),
            dma((line, halves)),
            dma((line, plane, halves)),
            dma((line, plane, halves)),
            dma((line, chain)),
            dma((2, line, chain)),
        ],
        compiler_params=pltpu.CompilerParams(
            collective_id=1, has_side_effects=True, vmem_limit_bytes=67043328
        ),
        name="layer",
    )(
        queries,
        keys,
        values,
        gates,
        decay,
        gain,
        project,
        residual,
        norm,
        ids,
        shares,
        *weights,
    )


def shards(
    queries,
    key_vectors,
    value_vectors,
    gate_inputs,
    log_decay,
    head_gain,
    out_weight,
    residual,
    norm_gain,
    expert_ids,
    expert_weights,
    gate_experts,
    up_experts,
    down_experts,
):
    return run_layer(
        (queries, key_vectors, value_vectors, gate_inputs, out_weight, residual),
        (log_decay.T, head_gain[None, :], norm_gain[None, :], expert_ids.T, expert_weights.T),
        (gate_experts, up_experts, down_experts),
        2 * queries.shape[0] // lax.axis_size("sp"),
    )


def solution(mesh):
    return jax.shard_map(
        shards,
        mesh=mesh,
        in_specs=(
            P("sp", "tp"),
            P("sp", "tp"),
            P("sp", "tp"),
            P("sp", "tp"),
            P("sp", "tp"),
            P("tp"),
            P("tp", None),
            P(("sp", "tp"), None),
            P(),
            P(("sp", "tp"), None),
            P(("sp", "tp"), None),
            P("sp", None, "tp"),
            P("sp", None, "tp"),
            P("sp", "tp", None),
        ),
        out_specs=P(("sp", "tp"), None),
        check_vma=False,
    )
```

```python
import functools

import jax
import jax.numpy as jnp
from jax import lax
from jax.experimental import pallas as pl
from jax.experimental.pallas import tpu as pltpu
from jax.sharding import PartitionSpec as P

MESH = pl.DeviceIdType.MESH


def line_length(count):
    size = 1
    while size * size * size < count:
        size *= 2
    return size


def layer_kernel(
    line,
    plane,
    cap,
    parts,
    halves,
    chain,
    query_hbm,
    key_hbm,
    value_hbm,
    gates_hbm,
    decay_ref,
    gain_ref,
    project_hbm,
    residual_hbm,
    norm_ref,
    ids_ref,
    shares_ref,
    gate_hbm,
    up_hbm,
    down_hbm,
    out_ref,
    query_ref,
    key_ref,
    value_ref,
    gates_ref,
    project_ref,
    residual_ref,
    cos_ref,
    sin_ref,
    running_ref,
    by_head_ref,
    turned_query,
    turned_key,
    start_query,
    within_ref,
    normed_ref,
    away_ref,
    got_ref,
    mixed_ref,
    meta_ref,
    state_out,
    state_in,
    totals,
    before_ref,
    plane_state,
    plane_total,
    line_state,
    line_total,
    carry_ref,
    back_state,
    start_state,
    lsem,
    osem,
    asend,
    arecv,
    bsend,
    brecv,
    ctsend,
    ctrecv,
    dsend,
    drecv,
    esend,
    erecv,
    gate_ref,
    up_ref,
    down_ref,
    zbuf,
    meta,
    sel,
    xbuf,
    hidden,
    ybuf,
    yin,
    sbuf,
    rbuf,
    cbuf,
    csend,
    pin,
    wsem,
    zsend,
    zrecv,
    msend,
    mrecv,
    psend,
    precv,
    tsend,
    trecv,
    ysend,
    yrecv,
    rsend,
    rrecv,
    ssend,
    srecv,
):
    sp, core = lax.axis_index("sp"), lax.axis_index("tp")
    z, p = sp // plane, lax.rem(sp, plane)
    length, channels = query_ref.shape
    tokens, width = residual_ref.shape
    lanes = cos_ref.shape[1]
    heads = decay_ref.shape[0]
    size = channels // heads
    pack = lanes // size
    groups = channels // lanes
    slice_rows = state_out.shape[1]
    slots = plane * cap
    f32, bf16 = jnp.float32, jnp.bfloat16

    def at(line_place, plane_place):
        return {"sp": line_place * plane + plane_place, "tp": core}

    partner = {"sp": sp, "tp": 1 - core}

    def remote(src, dst, send, recv, device):
        return pltpu.make_async_remote_copy(
            src_ref=src,
            dst_ref=dst,
            send_sem=send,
            recv_sem=recv,
            device_id=device,
            device_id_type=MESH,
        )

    def sent(ref, semaphore):
        remote(ref, ref, semaphore, semaphore, partner).wait_send()

    def came(ref, semaphore):
        remote(ref, ref, semaphore, semaphore, partner).wait_recv()

    others = pl.ds(0, plane - 1)
    loads = [
        pltpu.make_async_copy(source, target, lsem.at[number])
        for number, (source, target) in enumerate(
            (
                (query_hbm, query_ref),
                (key_hbm, key_ref),
                (value_hbm, value_ref),
                (gates_hbm, gates_ref),
                (project_hbm, project_ref),
                (residual_hbm, residual_ref),
            )
        )
    ]
    for copy in loads:
        copy.start()

    weights = [
        pltpu.make_async_copy(source.at[0], target, wsem.at[number])
        for number, (source, target) in enumerate(
            ((gate_hbm, gate_ref), (up_hbm, up_ref), (down_hbm, down_ref))
        )
    ]

    barrier = pltpu.get_barrier_semaphore()
    peers = [at(lax.rem(z + i, line), p) for i in range(1, line)]
    peers += [at(z, lax.rem(p + i, plane)) for i in range(1, plane)] + [partner]
    for peer in peers:
        pl.semaphore_signal(barrier, inc=1, device_id=peer, device_id_type=MESH)
    for copy in weights:
        copy.start()

    lane = lax.broadcasted_iota(jnp.int32, (1, lanes), 1)
    contract = (((1,), (1,)), ((), ()))
    upright = (((0,), (0,)), ((), ()))

    def place_of(group):
        return pl.ds(pl.multiple_of(group * lanes, lanes), lanes)

    def by_lane(pieces):
        value = pieces[-1]
        for number in range(pack - 2, -1, -1):
            value = jnp.where(lane < (number + 1) * size, pieces[number], value)
        return value

    with jax.named_scope("running"):
        rows_of = lax.broadcasted_iota(jnp.int32, (length, length), 0)
        columns_of = lax.broadcasted_iota(jnp.int32, (length, length), 1)
        causal = rows_of >= columns_of
        lower = jnp.where(causal, 1.0, 0.0).astype(bf16)
        upper = jnp.where(rows_of <= columns_of, 1.0, 0.0).astype(bf16)
        spread = lax.broadcasted_iota(jnp.int32, (heads, channels), 1) // size == (
            lax.broadcasted_iota(jnp.int32, (heads, channels), 0)
        )
        spread = jnp.where(spread, 1.0, 0.0).astype(bf16)
        rest = decay_ref[...]
        running, by_head = 0.0, 0.0
        for _ in range(3):
            piece = rest.astype(bf16)
            rest = rest - piece.astype(f32)
            wide_piece = lax.dot_general(piece, spread, upright, preferred_element_type=f32)
            wide_piece = wide_piece.astype(bf16)
            running = running + jnp.dot(lower, wide_piece, preferred_element_type=f32)
            by_head = by_head + jnp.dot(piece, upper, preferred_element_type=f32)
        running_ref[...] = running
        by_head_ref[...] = by_head

    swapped = lax.broadcasted_iota(jnp.int32, (lanes, lanes), 0) == (
        lax.broadcasted_iota(jnp.int32, (lanes, lanes), 1) ^ (size // 2)
    )
    swapped = jnp.where(swapped, 1.0, 0.0).astype(bf16)
    with jax.named_scope("table"):
        half_size = size // 2
        step_of = lane % half_size
        frequency = jnp.zeros((1, lanes), f32)
        for number in range(half_size):
            constant = float(10000.0 ** (-number / half_size))
            frequency = jnp.where(step_of == number, constant, frequency)
        fine = 16
        row = lax.broadcasted_iota(jnp.int32, (fine, lanes), 0)
        near_angle = row.astype(f32) * frequency
        near_cos, near_sin = jnp.cos(near_angle), jnp.sin(near_angle)
        rounds = length // fine
        row = lax.broadcasted_iota(jnp.int32, (rounds, lanes), 0)
        far_angle = (sp * length + row * fine).astype(f32) * frequency
        far_cos, far_sin = jnp.cos(far_angle), jnp.sin(far_angle)
        sign = jnp.where(lane % size < half_size, -1.0, 1.0)
        for number in range(rounds):
            some = pl.ds(number * fine, fine)
            a, b = far_cos[number : number + 1, :], far_sin[number : number + 1, :]
            cos_ref[some, :] = a * near_cos - b * near_sin
            sin_ref[some, :] = (b * near_cos + a * near_sin) * sign

    with jax.named_scope("loadw"):
        for copy in loads[:3]:
            copy.wait()

    def turn(block):
        other = jnp.dot(block, swapped, preferred_element_type=f32)
        return block.astype(f32) * cos_ref[...] + other * sin_ref[...]

    with jax.named_scope("turn"):
        for group in range(groups):
            where = pl.ds(group * lanes, lanes)
            run = running_ref[:, where]
            query = turn(query_ref[:, where])
            key = turn(key_ref[:, where]) * size ** (-0.5)
            turned_query[:, where] = query.astype(bf16)
            turned_key[:, where] = key.astype(bf16)
            start_query[:, where] = (query * jnp.exp(run)).astype(bf16)
            end = run[length - 1 : length, :]
            final = lax.dot_general(
                (key * jnp.exp(end - run)).astype(bf16),
                value_ref[:, where],
                upright,
                preferred_element_type=f32,
            )
            state = by_lane([final[n * size : (n + 1) * size, :] for n in range(pack)])
            totals[p, group] = jnp.broadcast_to(end, totals.shape[2:])
            per = size // slice_rows if slice_rows < size else 1
            deep = min(slice_rows, size)
            for part in range(per):
                row = group * size + part * deep
                state_out[row // slice_rows, pl.ds(row % slice_rows, deep), :] = state[
                    part * deep : (part + 1) * deep, :
                ].astype(bf16)
        state_in[p] = state_out[p]

    with jax.named_scope("barrier"):
        pl.semaphore_wait(barrier, len(peers))

    def state_copy(i):
        q = lax.rem(p + i, plane)
        return remote(
            state_out.at[q], state_in.at[p], asend.at[0], arecv.at[0], at(z, q)
        )

    def total_copy(i):
        q = lax.rem(p + i, plane)
        return remote(totals.at[p], totals.at[p], bsend.at[0], brecv.at[0], at(z, q))

    for i in range(1, plane):
        state_copy(i).start()
        total_copy(i).start()

    def meta_copy(i):
        return remote(
            meta_ref, meta.at[z], msend.at[0], mrecv.at[0], at(lax.rem(z + i, line), p)
        )

    count = line * plane
    with jax.named_scope("slots"):
        expert = lax.broadcasted_iota(jnp.int32, (count, tokens), 0).astype(f32)
        first, second = ids_ref[0:1, :].astype(f32), ids_ref[1:2, :].astype(f32)
        first_hot = jnp.where(expert == first, 1.0, 0.0)
        second_hot = jnp.where(expert == second, 1.0, 0.0)
        earlier = lax.broadcasted_iota(jnp.int32, (tokens, tokens), 0) < (
            lax.broadcasted_iota(jnp.int32, (tokens, tokens), 1)
        )
        taken = jnp.dot(
            (first_hot + second_hot).astype(bf16),
            jnp.where(earlier, 1.0, 0.0).astype(bf16),
            preferred_element_type=f32,
        )
        first_rank = jnp.sum(first_hot * taken, axis=0, keepdims=True)
        second_rank = jnp.sum(second_hot * taken, axis=0, keepdims=True)
        meta_ref[...] = jnp.zeros_like(meta_ref)
        meta_ref[0:1, :] = first * cap + first_rank
        meta_ref[1:2, :] = second * cap + second_rank
        meta_ref[2:4, :] = shares_ref[...]

    for i in range(1, line):
        meta_copy(i).start()

    def attend(lo, hi):
        @pl.loop(lo, hi)
        def _(group):
            where = place_of(group)
            query, key, value = turned_query[:, where], turned_key[:, where], value_ref[:, where]
            run = running_ref[:, where]
            total = []
            for number in range(pack):
                mine = (lane >= number * size) & (lane < (number + 1) * size)
                masked = jnp.where(mine, query, jnp.zeros_like(query))
                score = lax.dot_general(masked, key, contract, preferred_element_type=f32)
                gap = run[:, number * size : number * size + 1] - by_head_ref[
                    pl.ds(group * pack + number, 1), :
                ]
                ok = lax.broadcasted_iota(jnp.int32, (length, length), 0) >= (
                    lax.broadcasted_iota(jnp.int32, (length, length), 1)
                )
                weight = jnp.where(ok, jnp.exp(jnp.where(ok, gap, 0.0)), 0.0)
                total.append(
                    jnp.dot((score * weight).astype(bf16), value, preferred_element_type=f32)
                )
            within_ref[:, where] = by_lane(total)

    with jax.named_scope("attendA"):
        attend(0, groups // 2)

    mine = p * slice_rows // size
    with jax.named_scope("wait1"):
        came(state_in.at[others], arecv.at[0])
        came(totals.at[others], brecv.at[0])

    held = jnp.zeros((slice_rows, lanes), f32)
    elapsed = jnp.zeros((1, lanes), f32)
    for q in range(plane):
        before_ref[q] = held
        step = totals[q, mine][0:1, :]
        held = jnp.exp(step) * held + state_in[q].astype(f32)
        elapsed = elapsed + step
    plane_state[...] = held.astype(bf16)
    plane_total[...] = jnp.broadcast_to(elapsed, plane_total.shape)

    def line_state_copy(i):
        return remote(
            plane_state, line_state.at[z], ctsend.at[0], ctrecv.at[i, 0], at(z + i, p)
        )

    def line_total_copy(i):
        return remote(
            plane_total, line_total.at[z], ctsend.at[1], ctrecv.at[i, 1], at(z + i, p)
        )

    for i in range(1, line):

        @pl.when(z + i < line)
        def _():
            line_state_copy(i).start()
            line_total_copy(i).start()

    with jax.named_scope("attendB"):
        attend(groups // 2, groups)

    with jax.named_scope("wait2"):
        carry_ref[...] = jnp.zeros_like(carry_ref)
        for i in range(line - 1, 0, -1):

            @pl.when(z >= i)
            def _():
                line_state_copy(i).wait_recv()
                line_total_copy(i).wait_recv()
                step = line_total[z - i][0:1, :]
                carry_ref[...] = jnp.exp(step) * carry_ref[...] + line_state[z - i].astype(f32)

    elapsed = jnp.zeros((1, lanes), f32)
    for q in range(plane):
        value = before_ref[q] + jnp.exp(elapsed) * carry_ref[...]
        back_state[q] = value.astype(bf16)
        elapsed = elapsed + totals[q, mine][0:1, :]

    def start_copy(i):
        q = lax.rem(p + i, plane)
        return remote(
            back_state.at[q], start_state.at[p], dsend.at[0], drecv.at[0], at(z, q)
        )

    for i in range(1, plane):
        start_copy(i).start()
    start_state[p] = back_state[p]
    with jax.named_scope("wait3"):
        for copy in loads[3:]:
            copy.wait()
        came(start_state.at[others], drecv.at[0])

    with jax.named_scope("epilogue"):
        for group in range(groups):
            where = pl.ds(group * lanes, lanes)
            pieces = []
            for part in range(max(1, size // slice_rows)):
                row = group * size + part * slice_rows
                deep = min(slice_rows, size)
                pieces.append(start_state[row // slice_rows, pl.ds(row % slice_rows, deep), :])
            state = pieces[0] if len(pieces) == 1 else jnp.concatenate(pieces, axis=0)
            diagonal = jnp.concatenate(
                [
                    jnp.where(
                        (lane >= n * size) & (lane < (n + 1) * size), state, jnp.zeros_like(state)
                    )
                    for n in range(pack)
                ],
                axis=0,
            )
            retained = within_ref[:, where] + jnp.dot(
                start_query[:, where], diagonal, preferred_element_type=f32
            )
            square = retained * retained
            sums = [
                jnp.sum(
                    jnp.where((lane >= n * size) & (lane < (n + 1) * size), square, 0.0),
                    axis=1,
                    keepdims=True,
                )
                for n in range(pack)
            ]
            mean = by_lane(sums) * (1.0 / size)
            gates = gates_ref[:, where].astype(f32)
            normed = retained * lax.rsqrt(mean + 1e-06) * gain_ref[:, where]
            normed = normed * (gates / (1.0 + jnp.exp(-gates)))
            normed_ref[:, where] = normed.astype(bf16)

    def away_copy(h):
        columns = pl.ds(h * (width // 2), width // 2)
        return remote(
            away_ref.at[:, columns], got_ref.at[:, columns], esend.at[0], erecv.at[h], partner
        )

    away_rows = pl.ds(pl.multiple_of((1 - core) * tokens, tokens), tokens)
    here_rows = pl.ds(pl.multiple_of(core * tokens, tokens), tokens)
    with jax.named_scope("proj"):
        for h in range(2):
            columns = pl.ds(h * (width // 2), width // 2)
            away_ref[:, columns] = jnp.dot(
                normed_ref[away_rows, :], project_ref[:, columns], preferred_element_type=f32
            ).astype(bf16)
            away_copy(h).start()
        squares = jnp.zeros((tokens, 1), f32)
        for h in range(2):
            columns = pl.ds(h * (width // 2), width // 2)
            here = jnp.dot(
                normed_ref[here_rows, :], project_ref[:, columns], preferred_element_type=f32
            ).astype(bf16)
            away_copy(h).wait_recv()
            projected = here.astype(f32) + got_ref[:, columns].astype(f32)
            mixed = (residual_ref[:, columns].astype(f32) + projected).astype(bf16)
            mixed_ref[:, columns] = mixed
            mixed = mixed.astype(f32)
            squares = squares + jnp.sum(mixed * mixed, axis=1, keepdims=True)
        scale = lax.rsqrt(squares * (1.0 / width) + 1e-06)
        for h in range(2):
            columns = pl.ds(h * (width // 2), width // 2)
            normed = mixed_ref[:, columns].astype(f32) * scale * norm_ref[:, columns]
            zbuf[z, :, columns] = normed.astype(bf16)

    piece_rows = tokens // parts
    chain_width = width // chain

    def row_copy(way, block, part, target):
        rows = pl.ds(part * piece_rows, piece_rows)
        return remote(
            zbuf.at[block, rows],
            zbuf.at[block, rows],
            zsend.at[way],
            zrecv.at[block, part],
            at(target, p),
        )

    for part in range(parts):

        @pl.when(z + 1 < line)
        def _():
            row_copy(0, z, part, z + 1).start()

        @pl.when(z > 0)
        def _():
            row_copy(1, z, part, z - 1).start()

    meta[z] = meta_ref[...]

    near = jnp.minimum(z, line - 1 - z)
    longer_up = z < line - 1 - z

    def block_of(place):
        both = place <= 2 * near
        away = jnp.where(both, (place + 1) // 2, place - near)
        forward = jnp.where(both, place % 2 == 1, longer_up)
        return jnp.where(forward, z + away, z - away)

    def pass_on(distance, lo, hi):
        for part in range(lo, hi):
            low, high = z - distance, z + distance

            @pl.when(low >= 0)
            def _():
                row_copy(0, low, part, z).wait_recv()

                @pl.when(z + 1 < line)
                def _():
                    row_copy(0, low, part, z + 1).start()

            @pl.when(high < line)
            def _():
                row_copy(1, high, part, z).wait_recv()

                @pl.when(z > 0)
                def _():
                    row_copy(1, high, part, z - 1).start()

    def slot_names():
        names = lax.broadcasted_iota(jnp.int32, (slots, tokens), 0) + z * slots
        return names.astype(f32)

    def select_copy(j, i):
        q = lax.rem(p + i, plane)
        return remote(
            sel.at[j, q], xbuf.at[j, core, p], psend.at[0], precv.at[j, i], at(z, q)
        )

    def partner_copy(j, i):
        q = lax.rem(p + plane - i, plane)
        return remote(
            xbuf.at[j, core, q], xbuf.at[j, core, q], tsend.at[0], trecv.at[j], partner
        )

    def select(j):
        block = block_of(j)
        names = slot_names()
        chosen = (names == meta[block, 0:1, :]) | (names == meta[block, 1:2, :])
        place = jnp.where(chosen, 1.0, 0.0).astype(bf16)
        picked = jnp.dot(place, zbuf[block], preferred_element_type=f32)
        sel[j] = picked.reshape(plane, cap, width).astype(bf16)
        for i in range(1, plane):
            select_copy(j, i).start()
        xbuf[j, core, p] = sel[j, p]
        partner_copy(j, 0).start()

    def collect(j):
        for i in range(1, plane):
            select_copy(j, i).wait_recv()
            partner_copy(j, i).start()

    half = width // halves

    def partial_copy(j, h):
        columns = pl.ds(h * half, half)
        return remote(
            ybuf.at[j, 1 - core, :, :, columns],
            yin.at[j, :, :, columns],
            ysend.at[0],
            yrecv.at[j, h],
            partner,
        )

    tall = 2 * slots
    wide = 256

    def widen(j, lo, hi):
        if lo == hi:
            return
        if cap % 16 == 0:
            batch = xbuf[j].reshape(tall, width)
        else:
            batch = xbuf[j].astype(f32).reshape(tall, width).astype(bf16)

        for tile in range(lo, hi):
            columns = pl.ds(tile * wide, wide)
            gate = jnp.dot(batch, gate_ref[:, columns], preferred_element_type=f32)
            up = jnp.dot(batch, up_ref[:, columns], preferred_element_type=f32)
            hidden[:, columns] = (gate * up / (1.0 + jnp.exp(-gate))).astype(bf16)

    def narrow(j, h):
        for tile in range(h * (half // wide), (h + 1) * (half // wide)):
            columns = pl.ds(tile * wide, wide)
            value = jnp.dot(hidden[...], down_ref[:, columns], preferred_element_type=f32)
            ybuf[j, :, :, :, columns] = value.reshape(2, plane, cap, wide).astype(bf16)

        partial_copy(j, h).start()

    def return_copy(j, i, h):
        q = lax.rem(p + i, plane)
        columns = pl.ds(h * half, half)
        return remote(
            sbuf.at[j, q, :, columns],
            rbuf.at[j, p, :, columns],
            rsend.at[0],
            rrecv.at[j, h],
            at(z, q),
        )

    def give_back(j, h):
        columns = pl.ds(h * half, half)
        partial_copy(j, h).wait_recv()
        total = ybuf[j, core, :, :, columns].astype(f32) + yin[j, :, :, columns].astype(f32)
        sbuf[j, :, :, columns] = total.astype(bf16)
        for i in range(1, plane):
            return_copy(j, i, h).start()
        rbuf[j, p, :, columns] = sbuf[j, p, :, columns]

    def chain_copy(way, block, part, target):
        columns = pl.ds(part * chain_width, chain_width)
        lane_of = jnp.where((way == 1) & (block == target), line, block)
        return remote(
            csend.at[block, :, columns],
            pin.at[lane_of, :, columns],
            ssend.at[0],
            srecv.at[lane_of, part],
            at(target, p),
        )

    def weigh_of(j):
        block = block_of(j)
        names = slot_names()
        weigh = jnp.where(names == meta[block, 0:1, :], meta[block, 2:3, :], 0.0)
        weigh = weigh + jnp.where(names == meta[block, 1:2, :], meta[block, 3:4, :], 0.0)
        weigh = weigh.T
        high = weigh.astype(bf16)
        return high, (weigh - high.astype(f32)).astype(bf16)

    def combine(j, h, weigh):
        came(rbuf.at[j, others, :, pl.ds(h * half, half)], rrecv.at[j, h])
        block = block_of(j)
        high, low = weigh
        columns = pl.ds(h * half, half)
        if cap % 16 == 0:
            back = rbuf[j, :, :, columns].reshape(slots, half)
        else:
            back = rbuf[j, :, :, columns].astype(f32).reshape(slots, half).astype(bf16)
        total = jnp.dot(high, back, preferred_element_type=f32) + jnp.dot(
            low, back, preferred_element_type=f32
        )
        if j == 0:
            cbuf[block, :, columns] = total + mixed_ref[:, columns].astype(f32)
        else:
            cbuf[block, :, columns] = total

            @pl.when((z == 0) | (z == line - 1))
            def _():
                csend[block, :, columns] = total.astype(bf16)

            for part in range(h * chain // halves, (h + 1) * chain // halves):

                @pl.when(z == 0)
                def _():
                    chain_copy(0, block, part, z + 1).start()

                @pl.when(z == line - 1)
                def _():
                    chain_copy(1, block, part, z - 1).start()

    def relay(way, block, part):
        before = jnp.where(way == 0, z < block, z > block)
        inside = before & (z > 0) & (z < line - 1)
        columns = pl.ds(part * chain_width, chain_width)

        @pl.when(inside)
        def _():
            chain_copy(way, block, part, z).wait_recv()
            total = cbuf[block, :, columns] + pin[block, :, columns].astype(f32)
            csend[block, :, columns] = total.astype(bf16)
            chain_copy(way, block, part, z + 1 - 2 * way).start()

    first_way = jnp.where(2 * z < line, 0, 1)

    def relays(i, lo, hi):
        def one(way, part):
            relay(way, jnp.where(way == 0, i, line - 1 - i), part)

        for part in range(lo, hi + lag):
            if part < hi:
                one(first_way, part)
            if part >= lo + lag:
                one(1 - first_way, part - lag)

    lag = chain // 2
    tiles = hidden.shape[1] // wide
    sc = jax.named_scope
    with sc("select#0"):
        select(0)
    with sc("meta"):
        came(meta.at[pl.ds(0, line - 1)], mrecv.at[0])
    with sc("pass#1a"):
        pass_on(1, 0, parts // 2)
    with sc("collect#0"):
        collect(0)
    for j in range(line):
        last = j + 1 == line
        cut = tiles if last else tiles // 2 if j == 0 else 0
        with sc(f"xwait#{j}"):
            came(xbuf.at[j, 1 - core], trecv.at[j])
            if j == 0:
                for copy in weights:
                    copy.wait()
        with sc(f"widen#{j}a"):
            widen(j, 0, cut)
        if not last:
            with sc(f"pass#{j + 1}b"):
                pass_on(j + 1, parts // 2, parts)
            with sc(f"select#{j + 1}"):
                select(j + 1)
        with sc(f"widen#{j}b"):
            widen(j, cut, tiles)
        if j >= 2:
            with sc(f"combine#{j - 1}"):
                weigh = weigh_of(j - 1)
                for h in range(halves):
                    combine(j - 1, h, weigh)
        with sc(f"narrow#{j}a"):
            narrow(j, 0)
        with sc(f"narrow#{j}b"):
            for h in range(1, halves):
                narrow(j, h)
        if j + 2 < line:
            with sc(f"pass#{j + 2}a"):
                pass_on(j + 2, 0, parts // 2)
        if j >= 1:
            with sc(f"give#{j}"):
                for h in range(halves):
                    give_back(j, h)
        if j == max(0, line - 2):
            with sc("give#0"):
                for h in range(halves):
                    give_back(0, h)
        if not last:
            with sc(f"collect#{j + 1}"):
                collect(j + 1)
        if 2 <= j < line - 2:
            relays(j, 0, chain)
    weigh = weigh_of(line - 1)
    share = chain // halves
    for h in range(halves):
        if line > 2:
            with sc(f"relays#a{h}"):
                relays(line - 2, h * share, h * share + share // 2)
        with sc(f"combine#last{h}"):
            combine(line - 1, h, weigh)
        if line > 2:
            with sc(f"relays#b{h}"):
                relays(line - 2, h * share + share // 2, (h + 1) * share)
    with sc("relays#c"):
        relays(line - 1, 0, chain)
    with sc("combine#own"):
        weigh = weigh_of(0)
        for h in range(halves):
            combine(0, h, weigh)
    def out_copy(part):
        columns = pl.ds(part * chain_width, chain_width)
        return pltpu.make_async_copy(
            got_ref.at[:, columns], out_ref.at[:, columns], osem.at[0]
        )

    with sc("own"):
        for part in range(chain):
            columns = pl.ds(part * chain_width, chain_width)

            @pl.when(z > 0)
            def _():
                chain_copy(0, z, part, z).wait_recv()
                cbuf[z, :, columns] = cbuf[z, :, columns] + pin[z, :, columns].astype(f32)

            @pl.when(z < line - 1)
            def _():
                chain_copy(1, z, part, z).wait_recv()
                cbuf[z, :, columns] = cbuf[z, :, columns] + pin[line, :, columns].astype(f32)

            got_ref[:, columns] = cbuf[z, :, columns].astype(bf16)
            out_copy(part).start()

    with sc("store"):
        pltpu.make_async_copy(got_ref, out_ref, osem.at[0]).wait()

    with sc("drain"):
        sent(meta.at[pl.ds(0, line - 1)], msend.at[0])
        sent(state_out.at[others], asend.at[0])
        sent(totals.at[others], bsend.at[0])
        sent(back_state.at[others], dsend.at[0])
        sent(away_ref, esend.at[0])
        sent(sel.at[:, others], psend.at[0])
        sent(sel, tsend.at[0])
        sent(yin, ysend.at[0])
        sent(sbuf.at[:, others], rsend.at[0])
        sent(csend.at[pl.ds(0, line - 1)], ssend.at[0])
        for place in range(line):

            @pl.when(z == place)
            def _():
                if place + 1 < line:
                    sent(zbuf.at[pl.ds(0, place + 1)], zsend.at[0])
                    sent(line_state.at[pl.ds(0, line - 1 - place)], ctsend.at[0])
                    sent(line_total.at[pl.ds(0, line - 1 - place)], ctsend.at[1])
                if place > 0:
                    sent(zbuf.at[pl.ds(place, line - place)], zsend.at[1])


def run_layer(inputs, small, weights, cap):
    queries, keys, values, gates, project, residual = inputs
    decay, gain, norm, ids, shares = small
    lanes = 128
    count = lax.axis_size("sp")
    line = line_length(count)
    plane = count // line
    length, channels = queries.shape
    tokens, width = residual.shape
    heads = decay.shape[0]
    size = channels // heads
    groups = channels // lanes
    slice_rows = groups * size // plane
    inner = weights[0].shape[2]
    slots = plane * cap
    parts, halves, chain = 2, 2, 8
    bf16, f32 = jnp.bfloat16, jnp.float32
    dma = pltpu.SemaphoreType.DMA
    vmem = pl.BlockSpec(memory_space=pltpu.VMEM)
    hbm = pl.BlockSpec(memory_space=pl.ANY)
    return pl.pallas_call(
        functools.partial(layer_kernel, line, plane, cap, parts, halves, chain),
        out_shape=jax.ShapeDtypeStruct((tokens, width), bf16),
        in_specs=[hbm] * 4 + [vmem] * 2 + [hbm] * 2 + [vmem] * 3 + [hbm] * 3,
        out_specs=hbm,
        scratch_shapes=[
            pltpu.VMEM((length, channels), bf16),
            pltpu.VMEM((length, channels), bf16),
            pltpu.VMEM((length, channels), bf16),
            pltpu.VMEM((length, channels), bf16),
            pltpu.VMEM((channels, width), bf16),
            pltpu.VMEM((tokens, width), bf16),
            pltpu.VMEM((length, lanes), f32),
            pltpu.VMEM((length, lanes), f32),
            pltpu.VMEM((length, channels), f32),
            pltpu.VMEM((heads, length), f32),
            pltpu.VMEM((length, channels), bf16),
            pltpu.VMEM((length, channels), bf16),
            pltpu.VMEM((length, channels), bf16),
            pltpu.VMEM((length, channels), f32),
            pltpu.VMEM((length, channels), bf16),
            pltpu.VMEM((tokens, width), bf16),
            pltpu.VMEM((tokens, width), bf16),
            pltpu.VMEM((tokens, width), bf16),
            pltpu.VMEM((8, tokens), f32),
            pltpu.VMEM((plane, slice_rows, lanes), bf16),
            pltpu.VMEM((plane, slice_rows, lanes), bf16),
            pltpu.VMEM((plane, groups, 8, lanes), f32),
            pltpu.VMEM((plane, slice_rows, lanes), f32),
            pltpu.VMEM((slice_rows, lanes), bf16),
            pltpu.VMEM((8, lanes), f32),
            pltpu.VMEM((line, slice_rows, lanes), bf16),
            pltpu.VMEM((line, 8, lanes), f32),
            pltpu.VMEM((slice_rows, lanes), f32),
            pltpu.VMEM((plane, slice_rows, lanes), bf16),
            pltpu.VMEM((plane, slice_rows, lanes), bf16),
            dma((6,)),
            dma((1,)),
            dma((1,)),
            dma((1,)),
            dma((1,)),
            dma((1,)),
            dma((2,)),
            dma((line, 2)),
            dma((1,)),
            dma((1,)),
            dma((1,)),
            dma((2,)),
            pltpu.VMEM((width, inner), bf16),
            pltpu.VMEM((width, inner), bf16),
            pltpu.VMEM((inner, width), bf16),
            pltpu.VMEM((line, tokens, width), bf16),
            pltpu.VMEM((line, 8, tokens), f32),
            pltpu.VMEM((line, plane, cap, width), bf16),
            pltpu.VMEM((line, 2, plane, cap, width), bf16),
            pltpu.VMEM((2 * slots, inner), bf16),
            pltpu.VMEM((line, 2, plane, cap, width), bf16),
            pltpu.VMEM((line, plane, cap, width), bf16),
            pltpu.VMEM((line, plane, cap, width), bf16),
            pltpu.VMEM((line, plane, cap, width), bf16),
            pltpu.VMEM((line, tokens, width), f32),
            pltpu.VMEM((line, tokens, width), bf16),
            pltpu.VMEM((line + 1, tokens, width), bf16),
            dma((3,)),
            dma((2,)),
            dma((line, parts)),
            dma((1,)),
            dma((1,)),
            dma((1,)),
            dma((line, plane)),
            dma((1,)),
            dma((line,)),
            dma((1,)),
            dma((line, halves)),
            dma((1,)),
            dma((line, halves)),
            dma((1,)),
            dma((line + 1, chain)),
        ],
        compiler_params=pltpu.CompilerParams(
            collective_id=1, has_side_effects=True, vmem_limit_bytes=67043328
        ),
        name="layer",
    )(
        queries,
        keys,
        values,
        gates,
        decay,
        gain,
        project,
        residual,
        norm,
        ids,
        shares,
        *weights,
    )


def shards(
    queries,
    key_vectors,
    value_vectors,
    gate_inputs,
    log_decay,
    head_gain,
    out_weight,
    residual,
    norm_gain,
    expert_ids,
    expert_weights,
    gate_experts,
    up_experts,
    down_experts,
):
    return run_layer(
        (queries, key_vectors, value_vectors, gate_inputs, out_weight, residual),
        (log_decay.T, head_gain[None, :], norm_gain[None, :], expert_ids.T, expert_weights.T),
        (gate_experts, up_experts, down_experts),
        2 * queries.shape[0] // lax.axis_size("sp"),
    )


def solution(mesh):
    return jax.shard_map(
        shards,
        mesh=mesh,
        in_specs=(
            P("sp", "tp"),
            P("sp", "tp"),
            P("sp", "tp"),
            P("sp", "tp"),
            P("sp", "tp"),
            P("tp"),
            P("tp", None),
            P(("sp", "tp"), None),
            P(),
            P(("sp", "tp"), None),
            P(("sp", "tp"), None),
            P("sp", None, "tp"),
            P("sp", None, "tp"),
            P("sp", "tp", None),
        ),
        out_specs=P(("sp", "tp"), None),
        check_vma=False,
    )
```

```python
import functools

import jax
import jax.numpy as jnp
from jax import lax
from jax.experimental import pallas as pl
from jax.experimental.pallas import tpu as pltpu
from jax.sharding import PartitionSpec as P

MESH = pl.DeviceIdType.MESH


def line_length(count):
    size = 1
    while size * size * size < count:
        size *= 2
    return size


def layer_kernel(
    line,
    plane,
    cap,
    parts,
    halves,
    chain,
    query_hbm,
    key_hbm,
    value_hbm,
    gates_hbm,
    decay_hbm,
    gain_hbm,
    project_hbm,
    residual_hbm,
    norm_hbm,
    ids_hbm,
    shares_hbm,
    gate_hbm,
    up_hbm,
    down_hbm,
    out_ref,
    decay_ref,
    gain_ref,
    norm_ref,
    ids_ref,
    shares_ref,
    query_ref,
    key_ref,
    value_ref,
    gates_ref,
    project_ref,
    residual_ref,
    cos_ref,
    sin_ref,
    running_ref,
    by_head_ref,
    turned_query,
    turned_key,
    start_query,
    within_ref,
    normed_ref,
    away_ref,
    got_ref,
    mixed_ref,
    meta_ref,
    state_out,
    state_in,
    totals,
    before_ref,
    plane_state,
    plane_total,
    line_state,
    line_total,
    carry_ref,
    back_state,
    start_state,
    lsem,
    osem,
    asend,
    arecv,
    bsend,
    brecv,
    ctsend,
    ctrecv,
    dsend,
    drecv,
    esend,
    erecv,
    gate_ref,
    up_ref,
    down_ref,
    zbuf,
    meta,
    sel,
    xbuf,
    hidden,
    ybuf,
    yin,
    sbuf,
    rbuf,
    cbuf,
    csend,
    pin,
    wsem,
    zsend,
    zrecv,
    msend,
    mrecv,
    psend,
    precv,
    tsend,
    trecv,
    ysend,
    yrecv,
    rsend,
    rrecv,
    ssend,
    srecv,
):
    sp, core = lax.axis_index("sp"), lax.axis_index("tp")
    z, p = sp // plane, lax.rem(sp, plane)
    length, channels = query_ref.shape
    tokens, width = residual_ref.shape
    lanes = cos_ref.shape[1]
    heads = decay_ref.shape[0]
    size = channels // heads
    pack = lanes // size
    groups = channels // lanes
    slice_rows = state_out.shape[1]
    slots = plane * cap
    f32, bf16 = jnp.float32, jnp.bfloat16

    def at(line_place, plane_place):
        return {"sp": line_place * plane + plane_place, "tp": core}

    partner = {"sp": sp, "tp": 1 - core}

    def remote(src, dst, send, recv, device):
        return pltpu.make_async_remote_copy(
            src_ref=src,
            dst_ref=dst,
            send_sem=send,
            recv_sem=recv,
            device_id=device,
            device_id_type=MESH,
        )

    def sent(ref, semaphore):
        remote(ref, ref, semaphore, semaphore, partner).wait_send()

    def came(ref, semaphore):
        remote(ref, ref, semaphore, semaphore, partner).wait_recv()

    others = pl.ds(0, plane - 1)
    loads = [
        pltpu.make_async_copy(source, target, lsem.at[number])
        for number, (source, target) in enumerate(
            (
                (decay_hbm, decay_ref),
                (ids_hbm, ids_ref),
                (shares_hbm, shares_ref),
                (query_hbm, query_ref),
                (key_hbm, key_ref),
                (value_hbm, value_ref),
                (gates_hbm, gates_ref),
                (project_hbm, project_ref),
                (residual_hbm, residual_ref),
                (gain_hbm, gain_ref),
                (norm_hbm, norm_ref),
            )
        )
    ]
    for copy in loads:
        copy.start()

    weights = [
        pltpu.make_async_copy(source.at[0], target, wsem.at[number])
        for number, (source, target) in enumerate(
            ((gate_hbm, gate_ref), (up_hbm, up_ref), (down_hbm, down_ref))
        )
    ]

    barrier = pltpu.get_barrier_semaphore()
    peers = [at(lax.rem(z + i, line), p) for i in range(1, line)]
    peers += [at(z, lax.rem(p + i, plane)) for i in range(1, plane)] + [partner]
    for peer in peers:
        pl.semaphore_signal(barrier, inc=1, device_id=peer, device_id_type=MESH)
    for copy in weights:
        copy.start()

    lane = lax.broadcasted_iota(jnp.int32, (1, lanes), 1)
    contract = (((1,), (1,)), ((), ()))
    upright = (((0,), (0,)), ((), ()))

    def place_of(group):
        return pl.ds(pl.multiple_of(group * lanes, lanes), lanes)

    def by_lane(pieces):
        value = pieces[-1]
        for number in range(pack - 2, -1, -1):
            value = jnp.where(lane < (number + 1) * size, pieces[number], value)
        return value

    with jax.named_scope("table"):
        half_size = size // 2
        step_of = lane % half_size
        frequency = jnp.zeros((1, lanes), f32)
        for number in range(half_size):
            constant = float(10000.0 ** (-number / half_size))
            frequency = jnp.where(step_of == number, constant, frequency)
        fine = 16
        row = lax.broadcasted_iota(jnp.int32, (fine, lanes), 0)
        near_angle = row.astype(f32) * frequency
        near_cos, near_sin = jnp.cos(near_angle), jnp.sin(near_angle)
        rounds = length // fine
        row = lax.broadcasted_iota(jnp.int32, (rounds, lanes), 0)
        far_angle = (sp * length + row * fine).astype(f32) * frequency
        far_cos, far_sin = jnp.cos(far_angle), jnp.sin(far_angle)
        sign = jnp.where(lane % size < half_size, -1.0, 1.0)
        for number in range(rounds):
            some = pl.ds(number * fine, fine)
            a, b = far_cos[number : number + 1, :], far_sin[number : number + 1, :]
            cos_ref[some, :] = a * near_cos - b * near_sin
            sin_ref[some, :] = (b * near_cos + a * near_sin) * sign

    for copy in loads[:3]:
        copy.wait()

    with jax.named_scope("running"):
        rows_of = lax.broadcasted_iota(jnp.int32, (length, length), 0)
        columns_of = lax.broadcasted_iota(jnp.int32, (length, length), 1)
        causal = rows_of >= columns_of
        lower = jnp.where(causal, 1.0, 0.0).astype(bf16)
        upper = jnp.where(rows_of <= columns_of, 1.0, 0.0).astype(bf16)
        spread = lax.broadcasted_iota(jnp.int32, (heads, channels), 1) // size == (
            lax.broadcasted_iota(jnp.int32, (heads, channels), 0)
        )
        spread = jnp.where(spread, 1.0, 0.0).astype(bf16)
        rest = decay_ref[...]
        running, by_head = 0.0, 0.0
        for _ in range(3):
            piece = rest.astype(bf16)
            rest = rest - piece.astype(f32)
            wide_piece = lax.dot_general(piece, spread, upright, preferred_element_type=f32)
            wide_piece = wide_piece.astype(bf16)
            running = running + jnp.dot(lower, wide_piece, preferred_element_type=f32)
            by_head = by_head + jnp.dot(piece, upper, preferred_element_type=f32)
        running_ref[...] = running
        by_head_ref[...] = by_head

    swapped = lax.broadcasted_iota(jnp.int32, (lanes, lanes), 0) == (
        lax.broadcasted_iota(jnp.int32, (lanes, lanes), 1) ^ (size // 2)
    )
    swapped = jnp.where(swapped, 1.0, 0.0).astype(bf16)
    with jax.named_scope("loadw"):
        for copy in loads[3:6]:
            copy.wait()

    def turn(block):
        other = jnp.dot(block, swapped, preferred_element_type=f32)
        return block.astype(f32) * cos_ref[...] + other * sin_ref[...]

    with jax.named_scope("turn"):
        for group in range(groups):
            where = pl.ds(group * lanes, lanes)
            run = running_ref[:, where]
            query = turn(query_ref[:, where])
            key = turn(key_ref[:, where]) * size ** (-0.5)
            turned_query[:, where] = query.astype(bf16)
            turned_key[:, where] = key.astype(bf16)
            start_query[:, where] = (query * jnp.exp(run)).astype(bf16)
            end = run[length - 1 : length, :]
            final = lax.dot_general(
                (key * jnp.exp(end - run)).astype(bf16),
                value_ref[:, where],
                upright,
                preferred_element_type=f32,
            )
            state = by_lane([final[n * size : (n + 1) * size, :] for n in range(pack)])
            totals[p, group] = jnp.broadcast_to(end, totals.shape[2:])
            per = size // slice_rows if slice_rows < size else 1
            deep = min(slice_rows, size)
            for part in range(per):
                row = group * size + part * deep
                state_out[row // slice_rows, pl.ds(row % slice_rows, deep), :] = state[
                    part * deep : (part + 1) * deep, :
                ].astype(bf16)
        state_in[p] = state_out[p]

    with jax.named_scope("barrier"):
        pl.semaphore_wait(barrier, len(peers))

    def state_copy(i):
        q = lax.rem(p + i, plane)
        return remote(
            state_out.at[q], state_in.at[p], asend.at[0], arecv.at[0], at(z, q)
        )

    def total_copy(i):
        q = lax.rem(p + i, plane)
        return remote(totals.at[p], totals.at[p], bsend.at[0], brecv.at[0], at(z, q))

    for i in range(1, plane):
        state_copy(i).start()
        total_copy(i).start()

    def meta_copy(i):
        return remote(
            meta_ref, meta.at[z], msend.at[0], mrecv.at[0], at(lax.rem(z + i, line), p)
        )

    count = line * plane
    with jax.named_scope("slots"):
        expert = lax.broadcasted_iota(jnp.int32, (count, tokens), 0).astype(f32)
        first, second = ids_ref[0:1, :].astype(f32), ids_ref[1:2, :].astype(f32)
        first_hot = jnp.where(expert == first, 1.0, 0.0)
        second_hot = jnp.where(expert == second, 1.0, 0.0)
        earlier = lax.broadcasted_iota(jnp.int32, (tokens, tokens), 0) < (
            lax.broadcasted_iota(jnp.int32, (tokens, tokens), 1)
        )
        taken = jnp.dot(
            (first_hot + second_hot).astype(bf16),
            jnp.where(earlier, 1.0, 0.0).astype(bf16),
            preferred_element_type=f32,
        )
        first_rank = jnp.sum(first_hot * taken, axis=0, keepdims=True)
        second_rank = jnp.sum(second_hot * taken, axis=0, keepdims=True)
        meta_ref[...] = jnp.zeros_like(meta_ref)
        meta_ref[0:1, :] = first * cap + first_rank
        meta_ref[1:2, :] = second * cap + second_rank
        meta_ref[2:4, :] = shares_ref[...]

    for i in range(1, line):
        meta_copy(i).start()

    def attend(lo, hi):
        @pl.loop(lo, hi)
        def _(group):
            where = place_of(group)
            query, key, value = turned_query[:, where], turned_key[:, where], value_ref[:, where]
            run = running_ref[:, where]
            total = []
            for number in range(pack):
                mine = (lane >= number * size) & (lane < (number + 1) * size)
                masked = jnp.where(mine, query, jnp.zeros_like(query))
                score = lax.dot_general(masked, key, contract, preferred_element_type=f32)
                gap = run[:, number * size : number * size + 1] - by_head_ref[
                    pl.ds(group * pack + number, 1), :
                ]
                ok = lax.broadcasted_iota(jnp.int32, (length, length), 0) >= (
                    lax.broadcasted_iota(jnp.int32, (length, length), 1)
                )
                weight = jnp.where(ok, jnp.exp(jnp.where(ok, gap, 0.0)), 0.0)
                total.append(
                    jnp.dot((score * weight).astype(bf16), value, preferred_element_type=f32)
                )
            within_ref[:, where] = by_lane(total)

    with jax.named_scope("attendA"):
        attend(0, groups // 2)

    mine = p * slice_rows // size
    with jax.named_scope("wait1"):
        came(state_in.at[others], arecv.at[0])
        came(totals.at[others], brecv.at[0])

    held = jnp.zeros((slice_rows, lanes), f32)
    elapsed = jnp.zeros((1, lanes), f32)
    for q in range(plane):
        before_ref[q] = held
        step = totals[q, mine][0:1, :]
        held = jnp.exp(step) * held + state_in[q].astype(f32)
        elapsed = elapsed + step
    plane_state[...] = held.astype(bf16)
    plane_total[...] = jnp.broadcast_to(elapsed, plane_total.shape)

    def line_state_copy(i):
        return remote(
            plane_state, line_state.at[z], ctsend.at[0], ctrecv.at[i, 0], at(z + i, p)
        )

    def line_total_copy(i):
        return remote(
            plane_total, line_total.at[z], ctsend.at[1], ctrecv.at[i, 1], at(z + i, p)
        )

    for i in range(1, line):

        @pl.when(z + i < line)
        def _():
            line_state_copy(i).start()
            line_total_copy(i).start()

    with jax.named_scope("attendB"):
        attend(groups // 2, groups)

    with jax.named_scope("wait2"):
        carry_ref[...] = jnp.zeros_like(carry_ref)
        for i in range(line - 1, 0, -1):

            @pl.when(z >= i)
            def _():
                line_state_copy(i).wait_recv()
                line_total_copy(i).wait_recv()
                step = line_total[z - i][0:1, :]
                carry_ref[...] = jnp.exp(step) * carry_ref[...] + line_state[z - i].astype(f32)

    elapsed = jnp.zeros((1, lanes), f32)
    for q in range(plane):
        value = before_ref[q] + jnp.exp(elapsed) * carry_ref[...]
        back_state[q] = value.astype(bf16)
        elapsed = elapsed + totals[q, mine][0:1, :]

    def start_copy(i):
        q = lax.rem(p + i, plane)
        return remote(
            back_state.at[q], start_state.at[p], dsend.at[0], drecv.at[0], at(z, q)
        )

    for i in range(1, plane):
        start_copy(i).start()
    start_state[p] = back_state[p]
    with jax.named_scope("wait3"):
        for copy in loads[6:]:
            copy.wait()
        came(start_state.at[others], drecv.at[0])

    with jax.named_scope("epilogue"):
        for group in range(groups):
            where = pl.ds(group * lanes, lanes)
            pieces = []
            for part in range(max(1, size // slice_rows)):
                row = group * size + part * slice_rows
                deep = min(slice_rows, size)
                pieces.append(start_state[row // slice_rows, pl.ds(row % slice_rows, deep), :])
            state = pieces[0] if len(pieces) == 1 else jnp.concatenate(pieces, axis=0)
            diagonal = jnp.concatenate(
                [
                    jnp.where(
                        (lane >= n * size) & (lane < (n + 1) * size), state, jnp.zeros_like(state)
                    )
                    for n in range(pack)
                ],
                axis=0,
            )
            retained = within_ref[:, where] + jnp.dot(
                start_query[:, where], diagonal, preferred_element_type=f32
            )
            square = retained * retained
            sums = [
                jnp.sum(
                    jnp.where((lane >= n * size) & (lane < (n + 1) * size), square, 0.0),
                    axis=1,
                    keepdims=True,
                )
                for n in range(pack)
            ]
            mean = by_lane(sums) * (1.0 / size)
            gates = gates_ref[:, where].astype(f32)
            normed = retained * lax.rsqrt(mean + 1e-06) * gain_ref[:, where]
            normed = normed * (gates / (1.0 + jnp.exp(-gates)))
            normed_ref[:, where] = normed.astype(bf16)

    def away_copy(h):
        columns = pl.ds(h * (width // 2), width // 2)
        return remote(
            away_ref.at[:, columns], got_ref.at[:, columns], esend.at[0], erecv.at[h], partner
        )

    away_rows = pl.ds(pl.multiple_of((1 - core) * tokens, tokens), tokens)
    here_rows = pl.ds(pl.multiple_of(core * tokens, tokens), tokens)
    with jax.named_scope("proj"):
        for h in range(2):
            columns = pl.ds(h * (width // 2), width // 2)
            away_ref[:, columns] = jnp.dot(
                normed_ref[away_rows, :], project_ref[:, columns], preferred_element_type=f32
            ).astype(bf16)
            away_copy(h).start()
        squares = jnp.zeros((tokens, 1), f32)
        for h in range(2):
            columns = pl.ds(h * (width // 2), width // 2)
            here = jnp.dot(
                normed_ref[here_rows, :], project_ref[:, columns], preferred_element_type=f32
            ).astype(bf16)
            away_copy(h).wait_recv()
            projected = here.astype(f32) + got_ref[:, columns].astype(f32)
            mixed = (residual_ref[:, columns].astype(f32) + projected).astype(bf16)
            mixed_ref[:, columns] = mixed
            mixed = mixed.astype(f32)
            squares = squares + jnp.sum(mixed * mixed, axis=1, keepdims=True)
        scale = lax.rsqrt(squares * (1.0 / width) + 1e-06)
        for h in range(2):
            columns = pl.ds(h * (width // 2), width // 2)
            normed = mixed_ref[:, columns].astype(f32) * scale * norm_ref[:, columns]
            zbuf[z, :, columns] = normed.astype(bf16)

    piece_rows = tokens // parts
    chain_width = width // chain

    def row_copy(way, block, part, target):
        rows = pl.ds(part * piece_rows, piece_rows)
        return remote(
            zbuf.at[block, rows],
            zbuf.at[block, rows],
            zsend.at[way],
            zrecv.at[block, part],
            at(target, p),
        )

    for part in range(parts):

        @pl.when(z + 1 < line)
        def _():
            row_copy(0, z, part, z + 1).start()

        @pl.when(z > 0)
        def _():
            row_copy(1, z, part, z - 1).start()

    meta[z] = meta_ref[...]

    near = jnp.minimum(z, line - 1 - z)
    longer_up = z < line - 1 - z

    def block_of(place):
        both = place <= 2 * near
        away = jnp.where(both, (place + 1) // 2, place - near)
        forward = jnp.where(both, place % 2 == 1, longer_up)
        return jnp.where(forward, z + away, z - away)

    def pass_on(distance, lo, hi):
        for part in range(lo, hi):
            low, high = z - distance, z + distance

            @pl.when(low >= 0)
            def _():
                row_copy(0, low, part, z).wait_recv()

                @pl.when(z + 1 < line)
                def _():
                    row_copy(0, low, part, z + 1).start()

            @pl.when(high < line)
            def _():
                row_copy(1, high, part, z).wait_recv()

                @pl.when(z > 0)
                def _():
                    row_copy(1, high, part, z - 1).start()

    def slot_names():
        names = lax.broadcasted_iota(jnp.int32, (slots, tokens), 0) + z * slots
        return names.astype(f32)

    def select_copy(j, i):
        q = lax.rem(p + i, plane)
        return remote(
            sel.at[j, q], xbuf.at[j, core, p], psend.at[0], precv.at[j, i], at(z, q)
        )

    def partner_copy(j, i):
        q = lax.rem(p + plane - i, plane)
        return remote(
            xbuf.at[j, core, q], xbuf.at[j, core, q], tsend.at[0], trecv.at[j], partner
        )

    def select(j):
        block = block_of(j)
        names = slot_names()
        chosen = (names == meta[block, 0:1, :]) | (names == meta[block, 1:2, :])
        place = jnp.where(chosen, 1.0, 0.0).astype(bf16)
        picked = jnp.dot(place, zbuf[block], preferred_element_type=f32)
        sel[j] = picked.reshape(plane, cap, width).astype(bf16)
        for i in range(1, plane):
            select_copy(j, i).start()
        xbuf[j, core, p] = sel[j, p]
        partner_copy(j, 0).start()

    def collect(j):
        for i in range(1, plane):
            select_copy(j, i).wait_recv()
            partner_copy(j, i).start()

    half = width // halves

    def partial_copy(j, h):
        columns = pl.ds(h * half, half)
        return remote(
            ybuf.at[j, 1 - core, :, :, columns],
            yin.at[j, :, :, columns],
            ysend.at[0],
            yrecv.at[j, h],
            partner,
        )

    tall = 2 * slots
    wide = 256

    def widen(j, lo, hi):
        if lo == hi:
            return
        if cap % 16 == 0:
            batch = xbuf[j].reshape(tall, width)
        else:
            batch = xbuf[j].astype(f32).reshape(tall, width).astype(bf16)

        for tile in range(lo, hi):
            columns = pl.ds(tile * wide, wide)
            gate = jnp.dot(batch, gate_ref[:, columns], preferred_element_type=f32)
            up = jnp.dot(batch, up_ref[:, columns], preferred_element_type=f32)
            hidden[:, columns] = (gate * up / (1.0 + jnp.exp(-gate))).astype(bf16)

    def narrow(j, h):
        for tile in range(h * (half // wide), (h + 1) * (half // wide)):
            columns = pl.ds(tile * wide, wide)
            value = jnp.dot(hidden[...], down_ref[:, columns], preferred_element_type=f32)
            ybuf[j, :, :, :, columns] = value.reshape(2, plane, cap, wide).astype(bf16)

        partial_copy(j, h).start()

    def return_copy(j, i, h):
        q = lax.rem(p + i, plane)
        columns = pl.ds(h * half, half)
        return remote(
            sbuf.at[j, q, :, columns],
            rbuf.at[j, p, :, columns],
            rsend.at[0],
            rrecv.at[j, h],
            at(z, q),
        )

    def give_back(j, h):
        columns = pl.ds(h * half, half)
        partial_copy(j, h).wait_recv()
        total = ybuf[j, core, :, :, columns].astype(f32) + yin[j, :, :, columns].astype(f32)
        sbuf[j, :, :, columns] = total.astype(bf16)
        for i in range(1, plane):
            return_copy(j, i, h).start()
        rbuf[j, p, :, columns] = sbuf[j, p, :, columns]

    def chain_copy(way, block, part, target):
        columns = pl.ds(part * chain_width, chain_width)
        lane_of = jnp.where((way == 1) & (block == target), line, block)
        return remote(
            csend.at[block, :, columns],
            pin.at[lane_of, :, columns],
            ssend.at[0],
            srecv.at[lane_of, part],
            at(target, p),
        )

    def weigh_of(j):
        block = block_of(j)
        names = slot_names()
        weigh = jnp.where(names == meta[block, 0:1, :], meta[block, 2:3, :], 0.0)
        weigh = weigh + jnp.where(names == meta[block, 1:2, :], meta[block, 3:4, :], 0.0)
        weigh = weigh.T
        high = weigh.astype(bf16)
        return high, (weigh - high.astype(f32)).astype(bf16)

    def combine(j, h, weigh):
        came(rbuf.at[j, others, :, pl.ds(h * half, half)], rrecv.at[j, h])
        block = block_of(j)
        high, low = weigh
        columns = pl.ds(h * half, half)
        if cap % 16 == 0:
            back = rbuf[j, :, :, columns].reshape(slots, half)
        else:
            back = rbuf[j, :, :, columns].astype(f32).reshape(slots, half).astype(bf16)
        total = jnp.dot(high, back, preferred_element_type=f32) + jnp.dot(
            low, back, preferred_element_type=f32
        )
        if j == 0:
            cbuf[block, :, columns] = total + mixed_ref[:, columns].astype(f32)
        else:
            cbuf[block, :, columns] = total

            @pl.when((z == 0) | (z == line - 1))
            def _():
                csend[block, :, columns] = total.astype(bf16)

            for part in range(h * chain // halves, (h + 1) * chain // halves):

                @pl.when(z == 0)
                def _():
                    chain_copy(0, block, part, z + 1).start()

                @pl.when(z == line - 1)
                def _():
                    chain_copy(1, block, part, z - 1).start()

    def relay(way, block, part):
        before = jnp.where(way == 0, z < block, z > block)
        inside = before & (z > 0) & (z < line - 1)
        columns = pl.ds(part * chain_width, chain_width)

        @pl.when(inside)
        def _():
            chain_copy(way, block, part, z).wait_recv()
            total = cbuf[block, :, columns] + pin[block, :, columns].astype(f32)
            csend[block, :, columns] = total.astype(bf16)
            chain_copy(way, block, part, z + 1 - 2 * way).start()

    first_way = jnp.where(2 * z < line, 0, 1)

    def relays(i, lo, hi):
        def one(way, part):
            relay(way, jnp.where(way == 0, i, line - 1 - i), part)

        for part in range(lo, hi + lag):
            if part < hi:
                one(first_way, part)
            if part >= lo + lag:
                one(1 - first_way, part - lag)

    lag = chain // 2
    tiles = hidden.shape[1] // wide
    sc = jax.named_scope
    with sc("select#0"):
        select(0)
    with sc("meta"):
        came(meta.at[pl.ds(0, line - 1)], mrecv.at[0])
    with sc("pass#1a"):
        pass_on(1, 0, parts // 2)
    with sc("collect#0"):
        collect(0)
    for j in range(line):
        last = j + 1 == line
        cut = tiles if last else tiles // 2 if j == 0 else 0
        with sc(f"xwait#{j}"):
            came(xbuf.at[j, 1 - core], trecv.at[j])
            if j == 0:
                for copy in weights:
                    copy.wait()
        with sc(f"widen#{j}a"):
            widen(j, 0, cut)
        if not last:
            with sc(f"pass#{j + 1}b"):
                pass_on(j + 1, parts // 2, parts)
            with sc(f"select#{j + 1}"):
                select(j + 1)
        with sc(f"widen#{j}b"):
            widen(j, cut, tiles)
        if j >= 2:
            with sc(f"combine#{j - 1}"):
                weigh = weigh_of(j - 1)
                for h in range(halves):
                    combine(j - 1, h, weigh)
        with sc(f"narrow#{j}a"):
            narrow(j, 0)
        with sc(f"narrow#{j}b"):
            for h in range(1, halves):
                narrow(j, h)
        if j + 2 < line:
            with sc(f"pass#{j + 2}a"):
                pass_on(j + 2, 0, parts // 2)
        if j >= 1:
            with sc(f"give#{j}"):
                for h in range(halves):
                    give_back(j, h)
        if j == max(0, line - 2):
            with sc("give#0"):
                for h in range(halves):
                    give_back(0, h)
        if not last:
            with sc(f"collect#{j + 1}"):
                collect(j + 1)
        if 2 <= j < line - 2:
            relays(j, 0, chain)
    weigh = weigh_of(line - 1)
    share = chain // halves
    for h in range(halves):
        if line > 2:
            with sc(f"relays#a{h}"):
                relays(line - 2, h * share, h * share + share // 2)
        with sc(f"combine#last{h}"):
            combine(line - 1, h, weigh)
        if line > 2:
            with sc(f"relays#b{h}"):
                relays(line - 2, h * share + share // 2, (h + 1) * share)
    with sc("relays#c"):
        relays(line - 1, 0, chain)
    with sc("combine#own"):
        weigh = weigh_of(0)
        for h in range(halves):
            combine(0, h, weigh)
    def out_copy(part):
        columns = pl.ds(part * chain_width, chain_width)
        return pltpu.make_async_copy(
            got_ref.at[:, columns], out_ref.at[:, columns], osem.at[0]
        )

    with sc("own"):
        for part in range(chain):
            columns = pl.ds(part * chain_width, chain_width)

            @pl.when(z > 0)
            def _():
                chain_copy(0, z, part, z).wait_recv()
                cbuf[z, :, columns] = cbuf[z, :, columns] + pin[z, :, columns].astype(f32)

            @pl.when(z < line - 1)
            def _():
                chain_copy(1, z, part, z).wait_recv()
                cbuf[z, :, columns] = cbuf[z, :, columns] + pin[line, :, columns].astype(f32)

            got_ref[:, columns] = cbuf[z, :, columns].astype(bf16)
            out_copy(part).start()

    with sc("store"):
        pltpu.make_async_copy(got_ref, out_ref, osem.at[0]).wait()

    with sc("drain"):
        sent(meta.at[pl.ds(0, line - 1)], msend.at[0])
        sent(state_out.at[others], asend.at[0])
        sent(totals.at[others], bsend.at[0])
        sent(back_state.at[others], dsend.at[0])
        sent(away_ref, esend.at[0])
        sent(sel.at[:, others], psend.at[0])
        sent(sel, tsend.at[0])
        sent(yin, ysend.at[0])
        sent(sbuf.at[:, others], rsend.at[0])
        sent(csend.at[pl.ds(0, line - 1)], ssend.at[0])
        for place in range(line):

            @pl.when(z == place)
            def _():
                if place + 1 < line:
                    sent(zbuf.at[pl.ds(0, place + 1)], zsend.at[0])
                    sent(line_state.at[pl.ds(0, line - 1 - place)], ctsend.at[0])
                    sent(line_total.at[pl.ds(0, line - 1 - place)], ctsend.at[1])
                if place > 0:
                    sent(zbuf.at[pl.ds(place, line - place)], zsend.at[1])


def run_layer(inputs, small, weights, cap):
    queries, keys, values, gates, project, residual = inputs
    decay, gain, norm, ids, shares = small
    lanes = 128
    count = lax.axis_size("sp")
    line = line_length(count)
    plane = count // line
    length, channels = queries.shape
    tokens, width = residual.shape
    heads = decay.shape[0]
    size = channels // heads
    groups = channels // lanes
    slice_rows = groups * size // plane
    inner = weights[0].shape[2]
    slots = plane * cap
    parts, halves, chain = 2, 2, 16
    bf16, f32 = jnp.bfloat16, jnp.float32
    dma = pltpu.SemaphoreType.DMA
    hbm = pl.BlockSpec(memory_space=pl.ANY)
    return pl.pallas_call(
        functools.partial(layer_kernel, line, plane, cap, parts, halves, chain),
        out_shape=jax.ShapeDtypeStruct((tokens, width), bf16),
        in_specs=[hbm] * 14,
        out_specs=hbm,
        scratch_shapes=[
            pltpu.VMEM(decay.shape, decay.dtype),
            pltpu.VMEM(gain.shape, gain.dtype),
            pltpu.VMEM(norm.shape, norm.dtype),
            pltpu.VMEM(ids.shape, ids.dtype),
            pltpu.VMEM(shares.shape, shares.dtype),
            pltpu.VMEM((length, channels), bf16),
            pltpu.VMEM((length, channels), bf16),
            pltpu.VMEM((length, channels), bf16),
            pltpu.VMEM((length, channels), bf16),
            pltpu.VMEM((channels, width), bf16),
            pltpu.VMEM((tokens, width), bf16),
            pltpu.VMEM((length, lanes), f32),
            pltpu.VMEM((length, lanes), f32),
            pltpu.VMEM((length, channels), f32),
            pltpu.VMEM((heads, length), f32),
            pltpu.VMEM((length, channels), bf16),
            pltpu.VMEM((length, channels), bf16),
            pltpu.VMEM((length, channels), bf16),
            pltpu.VMEM((length, channels), f32),
            pltpu.VMEM((length, channels), bf16),
            pltpu.VMEM((tokens, width), bf16),
            pltpu.VMEM((tokens, width), bf16),
            pltpu.VMEM((tokens, width), bf16),
            pltpu.VMEM((8, tokens), f32),
            pltpu.VMEM((plane, slice_rows, lanes), bf16),
            pltpu.VMEM((plane, slice_rows, lanes), bf16),
            pltpu.VMEM((plane, groups, 8, lanes), f32),
            pltpu.VMEM((plane, slice_rows, lanes), f32),
            pltpu.VMEM((slice_rows, lanes), bf16),
            pltpu.VMEM((8, lanes), f32),
            pltpu.VMEM((line, slice_rows, lanes), bf16),
            pltpu.VMEM((line, 8, lanes), f32),
            pltpu.VMEM((slice_rows, lanes), f32),
            pltpu.VMEM((plane, slice_rows, lanes), bf16),
            pltpu.VMEM((plane, slice_rows, lanes), bf16),
            dma((11,)),
            dma((1,)),
            dma((1,)),
            dma((1,)),
            dma((1,)),
            dma((1,)),
            dma((2,)),
            dma((line, 2)),
            dma((1,)),
            dma((1,)),
            dma((1,)),
            dma((2,)),
            pltpu.VMEM((width, inner), bf16),
            pltpu.VMEM((width, inner), bf16),
            pltpu.VMEM((inner, width), bf16),
            pltpu.VMEM((line, tokens, width), bf16),
            pltpu.VMEM((line, 8, tokens), f32),
            pltpu.VMEM((line, plane, cap, width), bf16),
            pltpu.VMEM((line, 2, plane, cap, width), bf16),
            pltpu.VMEM((2 * slots, inner), bf16),
            pltpu.VMEM((line, 2, plane, cap, width), bf16),
            pltpu.VMEM((line, plane, cap, width), bf16),
            pltpu.VMEM((line, plane, cap, width), bf16),
            pltpu.VMEM((line, plane, cap, width), bf16),
            pltpu.VMEM((line, tokens, width), f32),
            pltpu.VMEM((line, tokens, width), bf16),
            pltpu.VMEM((line + 1, tokens, width), bf16),
            dma((3,)),
            dma((2,)),
            dma((line, parts)),
            dma((1,)),
            dma((1,)),
            dma((1,)),
            dma((line, plane)),
            dma((1,)),
            dma((line,)),
            dma((1,)),
            dma((line, halves)),
            dma((1,)),
            dma((line, halves)),
            dma((1,)),
            dma((line + 1, chain)),
        ],
        compiler_params=pltpu.CompilerParams(
            collective_id=1, has_side_effects=True, vmem_limit_bytes=67043328
        ),
        name="layer",
    )(
        queries,
        keys,
        values,
        gates,
        decay,
        gain,
        project,
        residual,
        norm,
        ids,
        shares,
        *weights,
    )


def shards(
    queries,
    key_vectors,
    value_vectors,
    gate_inputs,
    log_decay,
    head_gain,
    out_weight,
    residual,
    norm_gain,
    expert_ids,
    expert_weights,
    gate_experts,
    up_experts,
    down_experts,
):
    return run_layer(
        (queries, key_vectors, value_vectors, gate_inputs, out_weight, residual),
        (log_decay.T, head_gain[None, :], norm_gain[None, :], expert_ids.T, expert_weights.T),
        (gate_experts, up_experts, down_experts),
        2 * queries.shape[0] // lax.axis_size("sp"),
    )


def solution(mesh):
    return jax.shard_map(
        shards,
        mesh=mesh,
        in_specs=(
            P("sp", "tp"),
            P("sp", "tp"),
            P("sp", "tp"),
            P("sp", "tp"),
            P("sp", "tp"),
            P("tp"),
            P("tp", None),
            P(("sp", "tp"), None),
            P(),
            P(("sp", "tp"), None),
            P(("sp", "tp"), None),
            P("sp", None, "tp"),
            P("sp", None, "tp"),
            P("sp", "tp", None),
        ),
        out_specs=P(("sp", "tp"), None),
        check_vma=False,
    )
```
